512 devices in a mesh: ep: 32 (over z, x), tp: 16 (over y, core).
Axes of the slice: x: 4, y: 8, z: 8, core: 2. Of those that a mesh axis runs over, the one named last changes fastest.
Arguments:
- mix_input: bfloat16 [16384, 2048], P('ep', 'tp'), may hold values from -6 to 6
- mix_weight: bfloat16 [2048, 4096], P(None, 'tp'), may hold values from -0.125 to 0.125
- expert_input: bfloat16 [4096, 4096], P('ep', 'tp'), may hold values from -4500 to 4500
- expert_index: int32 [4096, 2], P('ep'), may hold values from 0 to 31, as said below
- route_share: float32 [4096, 2], P('ep'), may hold values from 0.1 to 1
- norm_gain: float32 [4096], replicated, may hold values from 0.1 to 1.9
- gate_weight: bfloat16 [32, 4096, 2048], P('ep', None, 'tp'), may hold values from -0.09375 to 0.09375
- up_weight: bfloat16 [32, 4096, 2048], P('ep', None, 'tp'), may hold values from -0.09375 to 0.09375
- down_weight: bfloat16 [32, 2048, 4096], P('ep', None, 'tp'), may hold values from -0.125 to 0.125
Outputs:
- mixed_rows: bfloat16 [16384, 4096], P('ep', 'tp')
- expert_rows: bfloat16 [4096, 4096], P('ep', 'tp')
The draws below stay inside these ranges and needn't reach their ends.
Inputs may be any that keep to these rules, and one draw needn't show every extreme that they name: `expert_index`: each row names 2 different experts. Within each aligned block of 128 rows (the rows of one index of ep) no expert is named by more than 16 rows, and one expert, the same in every block, is named by exactly 16 rows.
All inputs are finite; a program needn't handle non-finite values.
Results may differ from the reference program's by a relative error of at most 0.007.
Values may be sent and summed in bfloat16 or wider, within the bound.
A program may use at most 64 MiB of HBM per device.

```python
import math
from functools import partial
import jax
import jax.numpy as jnp
from jax import lax

D = 4096
POOL = 2048
FF = 2048
TOP = 2
TOK_EXP = 128
EXPERTS = 32
CAP = 16
TOKENS_MIX = 16384
TOKENS_EXP = 4096
N_EP = 32


def draw_expert_input(key, part):
    key_cols, key_rows, key_noise = jax.random.split(key, 3)
    column = jnp.arange(D, dtype=jnp.float32) / (D - 1)
    col_scale = jnp.exp(math.log(3.0) * column + jax.random.uniform(key_cols, (D,), jnp.float32, 0.0, math.log(10.0)))
    noise = jnp.clip(jax.random.normal(key_noise, (TOKENS_EXP, D), jnp.float32), -5.0, 5.0)
    row_scale = jnp.exp(jax.random.uniform(key_rows, (TOKENS_EXP, 1), jnp.float32, 0.0, math.log(10.0)))
    return (noise * col_scale[None, :] * row_scale).astype(jnp.bfloat16)


def draw_expert_index(key, part):
    key_full, key_rest = jax.random.split(key)
    favored = jax.random.randint(key_full, (), 0, EXPERTS)

    def one_block(block_key):
        key_order, key_rows, key_flip = jax.random.split(block_key, 3)
        others = jax.random.permutation(key_order, EXPERTS - 1).astype(jnp.int32)
        others = others + (others >= favored).astype(jnp.int32)
        row_number = jnp.arange(TOK_EXP, dtype=jnp.int32)
        first = jnp.where(row_number < CAP, favored, others[2 * row_number % (EXPERTS - 1)])
        second = jnp.where(row_number < CAP, others[row_number % (EXPERTS - 1)], others[(2 * row_number + 1) % (EXPERTS - 1)])
        flipped = jax.random.randint(key_flip, (TOK_EXP,), 0, 2)
        pairs = jnp.stack([jnp.where(flipped == 1, second, first), jnp.where(flipped == 1, first, second)], axis=1)
        shuffle = jax.random.permutation(key_rows, TOK_EXP)
        return pairs[shuffle]
    blocks = jax.vmap(one_block)(jax.random.split(key_rest, N_EP))
    return blocks.reshape(N_EP * TOK_EXP, 2).astype(jnp.int32)


def levels(own_key, shape, cuts, least, high):
    gain = 1.0
    for dim, shards_of in cuts:
        draws = jax.random.uniform(jax.random.fold_in(jax.random.fold_in(own_key, 6), dim), (shards_of,), jnp.float32, least / len(cuts), high / len(cuts))
        gain = gain * jnp.repeat(jnp.exp(draws), shape[dim] // shards_of).reshape((-1,) + (1,) * (len(shape) - 1 - dim))
    return gain


def normal_values(rng, shape, width, most, pieces=(), held_as=jnp.bfloat16):
    drawn = width * jax.random.normal(rng, shape, jnp.float32)
    if pieces:
        drawn = drawn * levels(rng, shape, pieces, -0.22, 0.18)
    return jnp.clip(drawn, -most, most).astype(held_as)


def setup_inputs(seed: int = 0) -> dict:
    key_of = jax.random.split(jax.random.key(seed), 10)
    mix_input = normal_values(key_of[0], (TOKENS_MIX, POOL), 1.0, 6.0, ((0, 32), (1, 16)))
    mix_weight = normal_values(key_of[1], (POOL, D), POOL ** -0.5, 0.125, ((1, 16),))
    expert_input = draw_expert_input(jax.random.fold_in(key_of[9], 71), 0)
    expert_index = draw_expert_index(jax.random.fold_in(key_of[9], 71), 0)
    route_share = jnp.clip(jnp.exp(math.log(1.0) - 2.3025851 * jax.random.uniform(key_of[4], (TOKENS_EXP, TOP), jnp.float32) ** levels(key_of[4], (TOKENS_EXP, TOP), ((0, 32),), -0.2, 0.2)), 0.1, 1.0)
    norm_gain = jnp.clip(1.0 + 0.18 * jax.random.normal(key_of[5], (D,), jnp.float32), 0.1, 1.9)
    gate_weight = normal_values(key_of[6], (EXPERTS, D, FF), D ** -0.5, 0.09375, ((0, 32), (2, 16)))
    up_weight = normal_values(key_of[7], (EXPERTS, D, FF), D ** -0.5, 0.09375, ((0, 32), (2, 16)))
    down_weight = normal_values(key_of[8], (EXPERTS, FF, D), FF ** -0.5, 0.125, ((0, 32), (2, 16)))
    return {"mix_input": mix_input, "mix_weight": mix_weight, "expert_input": expert_input, "expert_index": expert_index, "route_share": route_share, "norm_gain": norm_gain, "gate_weight": gate_weight, "up_weight": up_weight, "down_weight": down_weight}


window_reach = 15
norm_eps = 1e-06

def pool_minus_self(extended, first_pos, group_size, channel_base):
    length = extended.shape[0] - window_reach
    channels = extended.shape[1]
    channel = channel_base + jnp.arange(channels, dtype=jnp.int32)
    window = jnp.power(2, channel // group_size + 1).astype(jnp.int32)
    running = jnp.zeros((length, channels), jnp.float32)
    for lag_count in range(window_reach + 1):
        shifted = extended[window_reach - lag_count:window_reach - lag_count + length]
        running = running + jnp.where(lag_count < window[None, :], shifted, 0.0)
    position = first_pos + jnp.arange(length, dtype=jnp.int32)
    counts = jnp.minimum(position[:, None] + 1, window[None, :]).astype(jnp.float32)
    return (running / counts - extended[window_reach:]).astype(jnp.bfloat16)

def slot_targets(indices, experts, capacity):
    flattened = indices.reshape(-1)
    one_hot = (flattened[:, None] == jnp.arange(experts, dtype=jnp.int32)[None, :]).astype(jnp.int32)
    earlier = jnp.cumsum(one_hot, axis=0) - one_hot
    return flattened * capacity + lax.optimization_barrier(jnp.sum(earlier * one_hot, axis=1))

def reference(mix_input, mix_weight, expert_input, expert_index, route_share, norm_gain, gate_weight, up_weight, down_weight):
    extended = jnp.pad(mix_input.astype(jnp.float32), ((window_reach, 0), (0, 0)))
    pooled = pool_minus_self(extended, 0, POOL // 4, 0)
    mixed_rows = jnp.dot(pooled, mix_weight, preferred_element_type=jnp.float32).astype(jnp.bfloat16)
    blocks = expert_index.reshape(N_EP, TOK_EXP, TOP)
    targets = jax.vmap(partial(slot_targets, experts=EXPERTS, capacity=CAP))(blocks)
    expert_of = targets // CAP
    slot_of = targets % CAP
    source = jnp.arange(N_EP, dtype=jnp.int32)[:, None]
    placed = (expert_of * (N_EP * CAP) + source * CAP + slot_of).reshape(-1)
    row_ids = (source * TOK_EXP + jnp.repeat(jnp.arange(TOK_EXP, dtype=jnp.int32), TOP)[None, :]).reshape(-1)
    table = jnp.full((EXPERTS * N_EP * CAP,), TOKENS_EXP, jnp.int32).at[placed].set(row_ids)
    padded = jnp.concatenate([expert_input, jnp.zeros((1, D), jnp.bfloat16)], axis=0)

    def run_expert(operands):
        identity, gate_mat, up_mat, down_mat = operands
        rows_in = padded[identity]
        squares = lax.optimization_barrier(jnp.mean(jnp.square(rows_in.astype(jnp.float32)), axis=1, keepdims=True))
        inverse = lax.rsqrt(squares + norm_eps)
        scaled = (rows_in.astype(jnp.float32) * norm_gain).astype(jnp.bfloat16)
        gate_acts = jnp.dot(scaled, gate_mat, preferred_element_type=jnp.float32) * inverse
        up_acts = jnp.dot(scaled, up_mat, preferred_element_type=jnp.float32) * inverse
        hidden = (jax.nn.silu(gate_acts) * up_acts).astype(jnp.bfloat16)
        return jnp.dot(hidden, down_mat, preferred_element_type=jnp.float32).astype(jnp.bfloat16)
    produced = lax.map(run_expert, (table.reshape(EXPERTS, N_EP * CAP), gate_weight, up_weight, down_weight))
    picked = produced.reshape(EXPERTS * N_EP * CAP, D)[placed].astype(jnp.float32).reshape(TOKENS_EXP, TOP, D)
    shares = route_share / lax.optimization_barrier(jnp.sum(route_share, axis=1, keepdims=True))
    expert_rows = lax.optimization_barrier(jnp.sum(picked * shares[:, :, None], axis=1)).astype(jnp.bfloat16)
    return (mixed_rows, expert_rows)
```

```python
import functools

import jax
import jax.numpy as jnp
from jax import lax
from jax.experimental import pallas as pl
from jax.experimental.pallas import tpu as pltpu
from jax.sharding import PartitionSpec as P

MESH = pl.DeviceIdType.MESH
TOP = 2
REACH = 16
EPS = 1e-06
CHUNKS = 2
MIX_PIECES = 4


class Stream:
    def __init__(self, buf, pieces, groups, send, recv, mate_send, mate_recv):
        self.buf = buf
        self.pieces = pieces
        self.groups = groups
        self.per_group = pieces // groups
        self.rows = buf.shape[2] // pieces
        self.send, self.recv, self.mate_send, self.mate_recv = send, recv, mate_send, mate_recv


def kernel(
    ep_size,
    tp_size,
    group_size,
    order,
    mix_in,
    x_in,
    index_in,
    share_in,
    gain_in,
    mix_w,
    gate_w,
    up_w,
    down_w,
    mixed_out,
    rows_out,
    mw,
    wgu,
    wd,
    ext,
    halo,
    pg,
    tg,
    hg,
    outgoing,
    produced,
    returned,
    acc_m,
    acc_t,
    acc_d,
    squares,
    columns,
    w_sem,
    halo_sem,
    disp_send,
    disp_recv,
    ret_send,
    ret_recv,
    m_send,
    m_recv,
    m_mate_send,
    m_mate_recv,
    t_send,
    t_recv,
    t_mate_send,
    t_mate_recv,
    h_send,
    h_recv,
    h_mate_send,
    h_mate_recv,
):
    ep = lax.axis_index("ep")
    tp = lax.axis_index("tp")
    ny = tp_size // 2
    half = ny // 2
    core = lax.rem(tp, 2)
    y = tp // 2
    up = lax.rem(tp + 2, tp_size)
    down = lax.rem(tp + tp_size - 2, tp_size)
    mate = tp + 1 - 2 * core
    tokens, feats = x_in.shape
    length, chans = mix_in.shape
    slots = outgoing.shape[0]
    cap = slots // ep_size
    hid = hg.shape[3]
    chunk_rows = slots // CHUNKS
    in_chunk = ep_size // CHUNKS

    mix = Stream(pg, MIX_PIECES, 1, m_send, m_recv, m_mate_send, m_mate_recv)
    tok = Stream(tg, 2 * CHUNKS, CHUNKS, t_send, t_recv, t_mate_send, t_mate_recv)
    hdn = Stream(hg, 2 * CHUNKS, CHUNKS, h_send, h_recv, h_mate_send, h_mate_recv)

    def place(source):
        return lax.rem(source, CHUNKS) * in_chunk + source // CHUNKS

    def block(i):
        return pl.ds(pl.multiple_of(i * cap, cap), cap)

    w_copies = [
        pltpu.make_async_copy(mix_w, mw, w_sem.at[0]),
        pltpu.make_async_copy(gate_w, wgu.at[:, pl.ds(0, hid)], w_sem.at[1]),
        pltpu.make_async_copy(up_w, wgu.at[:, pl.ds(hid, hid)], w_sem.at[2]),
        pltpu.make_async_copy(down_w, wd, w_sem.at[3]),
    ]
    for copy in w_copies:
        copy.start()

    barrier = pltpu.get_barrier_semaphore()
    for other in (up, down, mate):
        pl.semaphore_signal(barrier, inc=1, device_id=(ep, other), device_id_type=MESH)

    def greet(i, carry):
        pl.semaphore_signal(
            barrier, inc=1, device_id=(lax.rem(ep + i, ep_size), tp), device_id_type=MESH
        )
        return carry

    lax.fori_loop(1, ep_size, greet, 0)

    expert_rows = lax.broadcasted_iota(jnp.int32, (ep_size, tokens), 0)
    named = [index_in[k : k + 1, :] for k in range(TOP)]
    hits = [(expert_rows == named[k]).astype(jnp.float32) for k in range(TOP)]
    before = (
        lax.broadcasted_iota(jnp.int32, (tokens, tokens), 0)
        < lax.broadcasted_iota(jnp.int32, (tokens, tokens), 1)
    ).astype(jnp.bfloat16)
    earlier = jnp.dot(
        (hits[0] + hits[1]).astype(jnp.bfloat16), before, preferred_element_type=jnp.float32
    )
    ranks = [
        jnp.sum(earlier * hits[0], axis=0, keepdims=True),
        jnp.sum((earlier + hits[0]) * hits[1], axis=0, keepdims=True),
    ]
    targets = [named[k] * cap + ranks[k].astype(jnp.int32) for k in range(TOP)]
    slot_rows = lax.broadcasted_iota(jnp.int32, (slots, tokens), 0)
    picks = jnp.logical_or(slot_rows == targets[0], slot_rows == targets[1])
    outgoing[...] = jnp.dot(
        picks.astype(jnp.bfloat16), x_in[...], preferred_element_type=jnp.float32
    ).astype(jnp.bfloat16)
    total_share = share_in[0:1, :] + share_in[1:2, :]
    row_id = lax.broadcasted_iota(jnp.int32, (tokens, tokens), 0)
    packed = jnp.zeros((tokens, tokens), jnp.float32)
    packed = jnp.where(row_id == 0, targets[0].astype(jnp.float32), packed)
    packed = jnp.where(row_id == 1, targets[1].astype(jnp.float32), packed)
    packed = jnp.where(row_id == 2, share_in[0:1, :] / total_share, packed)
    packed = jnp.where(row_id == 3, share_in[1:2, :] / total_share, packed)
    columns[...] = packed.T

    ext[pl.ds(REACH, length), :] = mix_in[...].astype(jnp.float32)
    group = (tp * chans) // group_size
    window = jnp.where(group == 0, 2, jnp.where(group == 1, 4, jnp.where(group == 2, 8, 16)))

    def window_sum(first, count):
        running = ext[pl.ds(REACH + first, count), :]
        for lag in range(1, REACH):
            running = running + jnp.where(
                lag < window, ext[pl.ds(REACH + first - lag, count), :], 0.0
            )
        return running

    inverse_window = jnp.where(
        group == 0, 0.5, jnp.where(group == 1, 0.25, jnp.where(group == 2, 0.125, 0.0625))
    )
    step = min(64, length // MIX_PIECES)
    for first in range(0, length, step):
        skip = REACH if first == 0 else 0
        at, count = first + skip, step - skip
        if count:
            pg[y, core, pl.ds(at, count), :] = (
                window_sum(at, count) * inverse_window - ext[pl.ds(REACH + at, count), :]
            ).astype(jnp.bfloat16)

    pl.semaphore_wait(barrier, ep_size - 1 + 3)

    halo_copy = pltpu.make_async_remote_copy(
        src_ref=mix_in.at[pl.ds(length - REACH, REACH), :],
        dst_ref=halo,
        send_sem=halo_sem.at[0],
        recv_sem=halo_sem.at[1],
        device_id=(lax.rem(ep + 1, ep_size), tp),
        device_id_type=MESH,
    )
    halo_copy.start()

    def dispatch(i, carry):
        other = lax.rem(ep + i, ep_size)
        pltpu.make_async_remote_copy(
            src_ref=outgoing.at[block(other), :],
            dst_ref=tg.at[y, core, block(place(ep)), :],
            send_sem=disp_send,
            recv_sem=disp_recv.at[lax.rem(ep, CHUNKS)],
            device_id=(other, tp),
            device_id_type=MESH,
        ).start()
        return carry

    def limit(piece, way):
        return half if (piece % 2 == 0) == (way == 0) else half - 1

    def part(stream, origin, piece):
        return stream.buf.at[origin, core, pl.ds(piece * stream.rows, stream.rows), :]

    def ring_send(stream, piece, way, origin, hop):
        ref = part(stream, origin, piece)
        pltpu.make_async_remote_copy(
            src_ref=ref,
            dst_ref=ref,
            send_sem=stream.send.at[piece],
            recv_sem=stream.recv.at[piece, way, hop],
            device_id=(ep, up if way == 0 else down),
            device_id_type=MESH,
        ).start()

    def mate_copy(stream, piece, origin, hop):
        ref = part(stream, origin, piece)
        pltpu.make_async_remote_copy(
            src_ref=ref,
            dst_ref=ref,
            send_sem=stream.mate_send.at[piece],
            recv_sem=stream.mate_recv.at[piece // stream.per_group, hop],
            device_id=(ep, mate),
            device_id_type=MESH,
        ).start()

    def origin_of(way, hop):
        return lax.rem(y + ny - hop, ny) if way == 0 else lax.rem(y + hop, ny)

    def move(stream, piece, hop):
        if hop == 0:
            for way in range(2):
                if limit(piece, way) > 0:
                    ring_send(stream, piece, way, y, 0)
            mate_copy(stream, piece, y, 0)
            return
        for way in range(2):
            if hop > limit(piece, way):
                continue
            origin = origin_of(way, hop)
            ref = part(stream, origin, piece)
            pltpu.make_async_copy(ref, ref, stream.recv.at[piece, way, hop - 1]).wait()
            if hop < limit(piece, way):
                ring_send(stream, piece, way, origin, hop)
            mate_copy(stream, piece, origin, hop)

    def mate_wait(stream, group_no, hop):
        rows = stream.rows * stream.per_group
        if 0 < hop < half:
            ref = stream.buf.at[pl.ds(0, 2), 0, pl.ds(0, rows), :]
        else:
            ref = stream.buf.at[0, 0, pl.ds(0, rows), :]
        pltpu.make_async_copy(ref, ref, stream.mate_recv.at[group_no, hop]).wait()

    def for_origins(hop, item):
        if hop == 0:
            item(y)
        elif hop == half:
            item(origin_of(0, hop))
        else:

            def both(way, carry):
                item(lax.rem(y + ny + (2 * way - 1) * hop, ny))
                return carry

            lax.fori_loop(0, 2, both, 0)

    def mix_item(first):
        def item(origin):
            a = jnp.concatenate([pg[origin, 0], pg[origin, 1]], axis=1)
            rows = pl.ds(pl.multiple_of(origin * 2 * chans, 2 * chans), 2 * chans)
            got = jnp.dot(a, mw[rows, :], preferred_element_type=jnp.float32)
            acc_m[...] = got if first else acc_m[...] + got

        return item

    def token_item(ch, first):
        at = pl.ds(ch * chunk_rows, chunk_rows)

        def item(origin):
            scaled, sums = [], 0.0
            for j in range(2):
                x = tg[origin, j, at, :].astype(jnp.float32)
                lanes = pl.ds(pl.multiple_of((origin * 2 + j) * feats, feats), feats)
                scaled.append((x * gain_in[:, lanes]).astype(jnp.bfloat16))
                sq = x * x
                for q in range(0, feats, 128):
                    sums = sums + sq[:, q : q + 128]
            rows = pl.ds(pl.multiple_of(origin * 2 * feats, 2 * feats), 2 * feats)
            got = jnp.dot(
                jnp.concatenate(scaled, axis=1), wgu[rows, :], preferred_element_type=jnp.float32
            )
            if first:
                acc_t[at, :] = got
                squares[at, :] = sums
            else:
                acc_t[at, :] = acc_t[at, :] + got
                squares[at, :] = squares[at, :] + sums

        return item

    def down_item(ch, first):
        at = pl.ds(ch * chunk_rows, chunk_rows)

        def item(origin):
            a = jnp.concatenate([hg[origin, 0, at, :], hg[origin, 1, at, :]], axis=1)
            rows = pl.ds(pl.multiple_of(origin * 2 * hid, 2 * hid), 2 * hid)
            got = jnp.dot(a, wd[rows, :], preferred_element_type=jnp.float32)
            acc_d[at, :] = got if first else acc_d[at, :] + got

        return item

    def activate(ch):
        at = pl.ds(ch * chunk_rows, chunk_rows)
        total = jnp.sum(squares[at, :], axis=1, keepdims=True)
        inverse = lax.rsqrt(total / (feats * tp_size) + EPS)
        gate = acc_t[at, pl.ds(0, hid)] * inverse
        upper = acc_t[at, pl.ds(hid, hid)] * inverse
        hg[y, core, at, :] = (gate / (1.0 + jnp.exp(-gate)) * upper).astype(jnp.bfloat16)

    def dispatched(ch):
        mine = lax.rem(ep, CHUNKS) == ch
        base = ch * chunk_rows

        @pl.when(mine)
        def _():
            if in_chunk > 1:
                ref = tg.at[0, 0, pl.ds(base, chunk_rows - cap), :]
                pltpu.make_async_copy(ref, ref, disp_recv.at[ch]).wait()
            tg[y, core, block(place(ep)), :] = outgoing[block(ep), :]

        @pl.when(jnp.logical_not(mine))
        def _():
            ref = tg.at[0, 0, pl.ds(base, chunk_rows), :]
            pltpu.make_async_copy(ref, ref, disp_recv.at[ch]).wait()

    def give_back(ch):
        at = pl.ds(ch * chunk_rows, chunk_rows)
        produced[at, :] = acc_d[at, :].astype(jnp.bfloat16)

        def one(i, carry):
            other = lax.rem(ep + i, ep_size)

            @pl.when(lax.rem(other, CHUNKS) == ch)
            def _():
                pltpu.make_async_remote_copy(
                    src_ref=produced.at[block(place(other)), :],
                    dst_ref=returned.at[block(ep), :],
                    send_sem=ret_send,
                    recv_sem=ret_recv,
                    device_id=(other, tp),
                    device_id_type=MESH,
                ).start()

            return carry

        lax.fori_loop(1, ep_size, one, 0)

        @pl.when(lax.rem(ep, CHUNKS) == ch)
        def _():
            returned[block(ep), :] = produced[block(place(ep)), :]

    def first_rows():
        halo_copy.wait_recv()
        ext[pl.ds(0, REACH), :] = jnp.where(ep == 0, 0.0, halo[...].astype(jnp.float32))
        position = ep * length + lax.broadcasted_iota(jnp.int32, (REACH, chans), 0)
        counts = jnp.minimum(position + 1, window).astype(jnp.float32)
        pg[y, core, pl.ds(0, REACH), :] = (
            window_sum(0, REACH) / counts - ext[pl.ds(REACH, REACH), :]
        ).astype(jnp.bfloat16)

    streams = {"m": mix, "t": tok, "h": hdn}
    for entry in order:
        kind = entry[0]
        if kind in streams:
            move(streams[kind], entry[1], entry[2])
        elif kind == "disp":
            lax.fori_loop(1, ep_size, dispatch, 0)
        elif kind == "first":
            first_rows()
        elif kind == "got":
            dispatched(entry[1])
        elif kind == "w":
            w_copies[entry[1]].wait()
        elif kind == "mc":
            mate_wait(mix, 0, entry[1])
            for_origins(entry[1], mix_item(entry[1] == 0))
        elif kind == "mo":
            mixed_out[...] = acc_m[...].astype(jnp.bfloat16)
        elif kind == "tc":
            mate_wait(tok, entry[1], entry[2])
            for_origins(entry[2], token_item(entry[1], entry[2] == 0))
        elif kind == "act":
            activate(entry[1])
        elif kind == "dc":
            mate_wait(hdn, entry[1], entry[2])
            for_origins(entry[2], down_item(entry[1], entry[2] == 0))
        elif kind == "ret":
            give_back(entry[1])

    halo_copy.wait_send()
    others = pl.ds(0, slots - cap)
    pltpu.make_async_copy(outgoing.at[others, :], outgoing.at[others, :], disp_send).wait()
    pltpu.make_async_copy(produced.at[others, :], produced.at[others, :], ret_send).wait()
    for stream in streams.values():
        for piece in range(stream.pieces):
            ref = stream.buf.at[pl.ds(0, ny - 1), 0, pl.ds(0, stream.rows), :]
            pltpu.make_async_copy(ref, ref, stream.send.at[piece]).wait()
            ref = stream.buf.at[pl.ds(0, ny), 0, pl.ds(0, stream.rows), :]
            pltpu.make_async_copy(ref, ref, stream.mate_send.at[piece]).wait()

    slot_lanes = lax.broadcasted_iota(jnp.int32, (tokens, slots), 1)
    takes = [
        (columns[:, k : k + 1].astype(jnp.int32) == slot_lanes).astype(jnp.bfloat16)
        for k in range(TOP)
    ]
    pltpu.make_async_copy(returned.at[others, :], returned.at[others, :], ret_recv).wait()
    rows = 0.0
    for k in range(TOP):
        picked = jnp.dot(takes[k], returned[...], preferred_element_type=jnp.float32)
        rows = rows + picked * columns[:, TOP + k : TOP + k + 1]
    rows_out[...] = rows.astype(jnp.bfloat16)


def full_order(half):
    m = [1, 2, 3, 0]
    order = [("m", 1, 0), ("m", 2, 0), ("m", 3, 0), ("disp",), ("first",), ("m", 0, 0)]
    for hop in (1, 2):
        order += [("m", p, hop) for p in m if hop <= half]
    order += [("got", 0), ("t", 0, 0), ("t", 1, 0)]
    for hop in range(3, half + 1):
        order += [("m", p, hop) for p in m]
    order += [("w", 0), ("mc", 0)]
    order += [("got", 1)]

    def t(ch, hop):
        return [("t", 2 * ch, hop), ("t", 2 * ch + 1, hop)]

    def h(ch, hop):
        return [("h", 2 * ch, hop), ("h", 2 * ch + 1, hop)]

    late = [("mc", hop) for hop in range(1, half + 1)] + [("mo",)]
    order += [("w", 1), ("w", 2)]
    if half == 4:
        order += t(0, 1) + [("t", 2, 0), late[0], ("tc", 0, 0)]
        order += t(0, 2) + [("t", 3, 0), late[1], ("tc", 0, 1)]
        order += t(0, 3) + [("t", 2, 1), late[2], ("tc", 0, 2)]
        order += t(0, 4) + [("t", 3, 1), ("tc", 0, 3), ("t", 2, 2), ("tc", 0, 4), ("act", 0)]
        order += [("h", 0, 0), ("h", 1, 0), ("t", 3, 2), ("tc", 1, 0), ("h", 0, 1), ("t", 2, 3)]
        order += [("h", 1, 1), ("t", 3, 3), late[3], late[4], ("tc", 1, 1), ("w", 3), ("dc", 0, 0)]
        order += h(0, 2) + [("tc", 1, 2), ("dc", 0, 1)] + t(1, 4)
        order += [("tc", 1, 3)] + h(0, 3) + [("tc", 1, 4), ("act", 1)]
        order += h(1, 0) + [("dc", 0, 2)] + h(0, 4) + h(1, 1)
        order += [("dc", 0, 3), ("dc", 0, 4), ("ret", 0)]
        order += h(1, 2) + [("dc", 1, 0)] + h(1, 3) + [("dc", 1, 1)] + h(1, 4)
        order += [("dc", 1, 2), ("dc", 1, 3), ("dc", 1, 4), ("ret", 1)]
    else:
        order += t(1, 0)
        for ch in range(CHUNKS):
            for hop in range(1, half + 1):
                order += t(ch, hop)
            order += [("tc", ch, hop) for hop in range(half + 1)] + [("act", ch)]
        order += late + [("w", 3)]
        for ch in range(CHUNKS):
            order += h(ch, 0)
        for ch in range(CHUNKS):
            for hop in range(1, half + 1):
                order += h(ch, hop)
            order += [("dc", ch, hop) for hop in range(half + 1)] + [("ret", ch)]
    return order


def solution(mesh):
    ep_size, tp_size = mesh.shape["ep"], mesh.shape["tp"]
    ny = tp_size // 2
    half = ny // 2

    def shards(mix_input, mix_weight, expert_input, expert_index, route_share, norm_gain, gate_weight, up_weight, down_weight):
        length, chans = mix_input.shape
        tokens, feats = expert_input.shape
        slots = 2 * tokens * TOP
        width = mix_weight.shape[1]
        hid = gate_weight.shape[2]
        vmem, dma = pltpu.VMEM, pltpu.SemaphoreType.DMA
        bf16, f32 = jnp.bfloat16, jnp.float32

        def stream_sems(pieces, groups):
            return [dma((pieces,)), dma((pieces, 2, half)), dma((pieces,)), dma((groups, half + 1))]

        here = pl.BlockSpec(memory_space=pltpu.VMEM)
        there = pl.BlockSpec(memory_space=pl.ANY)
        flops = 2 * (length * chans * tp_size * width + slots * (feats * tp_size * 2 * hid + hid * tp_size * width))
        call = pl.pallas_call(
            functools.partial(
                kernel, ep_size, tp_size, chans * tp_size // 4, full_order(half)
            ),
            name="mixer_and_experts",
            out_shape=(
                jax.ShapeDtypeStruct((length, width), bf16),
                jax.ShapeDtypeStruct((tokens, width), bf16),
            ),
            in_specs=[here] * 5 + [there] * 4,
            out_specs=(here, here),
            scratch_shapes=[
                vmem(mix_weight.shape, bf16),
                vmem((feats * tp_size, 2 * hid), bf16),
                vmem(down_weight.shape[1:], bf16),
                vmem((length + REACH, chans), f32),
                vmem((REACH, chans), bf16),
                vmem((ny, 2, length, chans), bf16),
                vmem((ny, 2, slots, feats), bf16),
                vmem((ny, 2, slots, hid), bf16),
                vmem((slots, feats), bf16),
                vmem((slots, width), bf16),
                vmem((slots, width), bf16),
                vmem((length, width), f32),
                vmem((slots, 2 * hid), f32),
                vmem((slots, width), f32),
                vmem((slots, 128), f32),
                vmem((tokens, tokens), f32),
                dma((4,)),
                dma((2,)),
                dma,
                dma((CHUNKS,)),
                dma,
                dma,
            ]
            + stream_sems(MIX_PIECES, 1)
            + stream_sems(2 * CHUNKS, CHUNKS)
            + stream_sems(2 * CHUNKS, CHUNKS),
            compiler_params=pltpu.CompilerParams(
                collective_id=0, has_side_effects=True, vmem_limit_bytes=60 * 1024 * 1024
            ),
            cost_estimate=pl.CostEstimate(flops=flops, bytes_accessed=8 * 1024 * 1024, transcendentals=0),
        )
        return call(
            mix_input,
            expert_input,
            expert_index.T,
            route_share.T,
            norm_gain.reshape(1, -1),
            mix_weight,
            gate_weight[0],
            up_weight[0],
            down_weight[0],
        )

    placed = (
        P("ep", "tp"),
        P(None, "tp"),
        P("ep", "tp"),
        P("ep", None),
        P("ep", None),
        P(),
        P("ep", None, "tp"),
        P("ep", None, "tp"),
        P("ep", None, "tp"),
    )
    return jax.shard_map(
        shards,
        mesh=mesh,
        in_specs=placed,
        out_specs=(P("ep", "tp"), P("ep", "tp")),
        check_vma=False,
    )
```

```python
import functools

import jax
import jax.numpy as jnp
from jax import lax
from jax.experimental import pallas as pl
from jax.experimental.pallas import tpu as pltpu
from jax.sharding import PartitionSpec as P

MESH = pl.DeviceIdType.MESH
TOP = 2
REACH = 16
EPS = 1e-06
MIX_GROUPS = 2


class Stream:
    def __init__(self, buf, group_rows, sems):
        self.buf = buf
        self.group_rows = group_rows
        self.group_first = [sum(group_rows[:g]) for g in range(len(group_rows))]
        self.send, self.recv, self.mate_send, self.mate_recv = sems

    def group(self, g):
        return pl.ds(self.group_first[g], self.group_rows[g])

    def rows(self, piece):
        size = self.group_rows[piece // 2] // 2
        return self.group_first[piece // 2] + (piece % 2) * size, size


def kernel(
    ep_size,
    tp_size,
    group_size,
    sources,
    order,
    mix_hbm,
    x_hbm,
    index_hbm,
    share_hbm,
    gain_hbm,
    mix_w,
    gate_w,
    up_w,
    down_w,
    mixed_out,
    rows_out,
    mix_in,
    x_in,
    index_in,
    share_in,
    gain_in,
    mw,
    wgu,
    wd,
    ext,
    halo,
    pg,
    tg,
    hg,
    outgoing,
    produced,
    returned,
    acc_m,
    acc_t,
    acc_d,
    squares,
    columns,
    in_sem,
    w_sem,
    halo_sem,
    disp_send,
    disp_recv,
    ret_send,
    ret_recv,
    m_send,
    m_recv,
    m_mate_send,
    m_mate_recv,
    t_send,
    t_recv,
    t_mate_send,
    t_mate_recv,
    h_send,
    h_recv,
    h_mate_send,
    h_mate_recv,
):
    ep = lax.axis_index("ep")
    tp = lax.axis_index("tp")
    ny = tp_size // 2
    half = ny // 2
    core = lax.rem(tp, 2)
    y = tp // 2
    up = lax.rem(tp + 2, tp_size)
    down = lax.rem(tp + tp_size - 2, tp_size)
    mate = tp + 1 - 2 * core
    tokens, feats = x_in.shape
    length, chans = mix_in.shape
    slots = outgoing.shape[0]
    cap = slots // ep_size
    hid = hg.shape[3]
    chunks = [n * cap for n in sources]
    bounds = [sum(sources[:ch]) for ch in range(len(sources) + 1)]

    mix = Stream(pg, [length // MIX_GROUPS] * MIX_GROUPS, (m_send, m_recv, m_mate_send, m_mate_recv))
    tok = Stream(tg, chunks, (t_send, t_recv, t_mate_send, t_mate_recv))
    hdn = Stream(hg, chunks, (h_send, h_recv, h_mate_send, h_mate_recv))

    def block(i):
        return pl.ds(pl.multiple_of(i * cap, cap), cap)

    in_copies = [
        pltpu.make_async_copy(src, dst, in_sem.at[i])
        for i, (src, dst) in enumerate(
            (
                (index_hbm, index_in),
                (x_hbm, x_in),
                (share_hbm, share_in),
                (mix_hbm, mix_in),
                (gain_hbm, gain_in),
            )
        )
    ]
    for copy in in_copies:
        copy.start()
    w_copies = [
        pltpu.make_async_copy(mix_w, mw, w_sem.at[0]),
        pltpu.make_async_copy(gate_w, wgu.at[:, pl.ds(0, hid)], w_sem.at[1]),
        pltpu.make_async_copy(up_w, wgu.at[:, pl.ds(hid, hid)], w_sem.at[2]),
        pltpu.make_async_copy(down_w, wd, w_sem.at[3]),
    ]
    for copy in w_copies:
        copy.start()

    barrier = pltpu.get_barrier_semaphore()
    for other in (up, down, mate):
        pl.semaphore_signal(barrier, inc=1, device_id=(ep, other), device_id_type=MESH)

    def greet(i, carry):
        pl.semaphore_signal(
            barrier, inc=1, device_id=(lax.rem(ep + i, ep_size), tp), device_id_type=MESH
        )
        return carry

    lax.fori_loop(1, ep_size, greet, 0)

    for copy in in_copies:
        copy.wait()

    expert_rows = lax.broadcasted_iota(jnp.int32, (ep_size, tokens), 0)
    named = [index_in[k : k + 1, :] for k in range(TOP)]
    hits = [(expert_rows == named[k]).astype(jnp.float32) for k in range(TOP)]
    before = (
        lax.broadcasted_iota(jnp.int32, (tokens, tokens), 0)
        < lax.broadcasted_iota(jnp.int32, (tokens, tokens), 1)
    ).astype(jnp.bfloat16)
    earlier = jnp.dot(
        (hits[0] + hits[1]).astype(jnp.bfloat16), before, preferred_element_type=jnp.float32
    )
    ranks = [
        jnp.sum(earlier * hits[0], axis=0, keepdims=True),
        jnp.sum((earlier + hits[0]) * hits[1], axis=0, keepdims=True),
    ]
    targets = [named[k] * cap + ranks[k].astype(jnp.int32) for k in range(TOP)]
    slot_rows = lax.broadcasted_iota(jnp.int32, (slots, tokens), 0)
    picks = jnp.logical_or(slot_rows == targets[0], slot_rows == targets[1])
    outgoing[...] = jnp.dot(
        picks.astype(jnp.bfloat16), x_in[...], preferred_element_type=jnp.float32
    ).astype(jnp.bfloat16)
    total_share = share_in[0:1, :] + share_in[1:2, :]
    row_id = lax.broadcasted_iota(jnp.int32, (tokens, tokens), 0)
    packed = jnp.zeros((tokens, tokens), jnp.float32)
    packed = jnp.where(row_id == 0, targets[0].astype(jnp.float32), packed)
    packed = jnp.where(row_id == 1, targets[1].astype(jnp.float32), packed)
    packed = jnp.where(row_id == 2, share_in[0:1, :] / total_share, packed)
    packed = jnp.where(row_id == 3, share_in[1:2, :] / total_share, packed)
    columns[...] = packed.T

    ext[pl.ds(REACH, length), :] = mix_in[...].astype(jnp.float32)
    group = (tp * chans) // group_size
    window = jnp.where(group == 0, 2, jnp.where(group == 1, 4, jnp.where(group == 2, 8, 16)))

    def window_sum(first, count):
        running = ext[pl.ds(REACH + first, count), :]
        for lag in range(1, REACH):
            running = running + jnp.where(
                lag < window, ext[pl.ds(REACH + first - lag, count), :], 0.0
            )
        return running

    inverse_window = jnp.where(
        group == 0, 0.5, jnp.where(group == 1, 0.25, jnp.where(group == 2, 0.125, 0.0625))
    )
    def pool(piece):
        at, size = mix.rows(piece)
        for first in range(at, at + size, min(64, size)):
            skip = REACH if first == 0 else 0
            begin, count = first + skip, min(64, size) - skip
            if count:
                pg[y, core, pl.ds(begin, count), :] = (
                    window_sum(begin, count) * inverse_window - ext[pl.ds(REACH + begin, count), :]
                ).astype(jnp.bfloat16)

    pl.semaphore_wait(barrier, ep_size - 1 + 3)

    halo_copy = pltpu.make_async_remote_copy(
        src_ref=mix_in.at[pl.ds(length - REACH, REACH), :],
        dst_ref=halo,
        send_sem=halo_sem.at[0],
        recv_sem=halo_sem.at[1],
        device_id=(lax.rem(ep + 1, ep_size), tp),
        device_id_type=MESH,
    )
    halo_copy.start()

    my_chunk = 0
    for bound in bounds[1:-1]:
        my_chunk = my_chunk + jnp.where(ep >= bound, 1, 0)

    def dispatch(i, carry):
        other = lax.rem(ep + i, ep_size)
        pltpu.make_async_remote_copy(
            src_ref=outgoing.at[block(other), :],
            dst_ref=tg.at[y, core, block(ep), :],
            send_sem=disp_send,
            recv_sem=disp_recv.at[my_chunk],
            device_id=(other, tp),
            device_id_type=MESH,
        ).start()
        return carry

    def limit(piece, way):
        return half if (piece % 2 == 0) == (way == 0) else half - 1

    def part(stream, origin, piece):
        return stream.buf.at[origin, core, pl.ds(*stream.rows(piece)), :]

    def ring_send(stream, piece, way, origin, hop):
        ref = part(stream, origin, piece)
        pltpu.make_async_remote_copy(
            src_ref=ref,
            dst_ref=ref,
            send_sem=stream.send.at[piece],
            recv_sem=stream.recv.at[piece, way, hop],
            device_id=(ep, up if way == 0 else down),
            device_id_type=MESH,
        ).start()

    def mate_copy(stream, piece, origin, hop):
        ref = part(stream, origin, piece)
        pltpu.make_async_remote_copy(
            src_ref=ref,
            dst_ref=ref,
            send_sem=stream.mate_send.at[piece],
            recv_sem=stream.mate_recv.at[piece // 2, hop],
            device_id=(ep, mate),
            device_id_type=MESH,
        ).start()

    def origin_of(way, hop):
        return lax.rem(y + ny - hop, ny) if way == 0 else lax.rem(y + hop, ny)

    def move(stream, piece, hop):
        if hop == 0:
            for way in range(2):
                if limit(piece, way) > 0:
                    ring_send(stream, piece, way, y, 0)
            mate_copy(stream, piece, y, 0)
            return
        for way in range(2):
            if hop > limit(piece, way):
                continue
            origin = origin_of(way, hop)
            ref = part(stream, origin, piece)
            pltpu.make_async_copy(ref, ref, stream.recv.at[piece, way, hop - 1]).wait()
            if hop < limit(piece, way):
                ring_send(stream, piece, way, origin, hop)
            mate_copy(stream, piece, origin, hop)

    def mate_wait(stream, group_no, hop):
        rows = stream.group_rows[group_no]
        if 0 < hop < half:
            ref = stream.buf.at[pl.ds(0, 2), 0, pl.ds(0, rows), :]
        else:
            ref = stream.buf.at[0, 0, pl.ds(0, rows), :]
        pltpu.make_async_copy(ref, ref, stream.mate_recv.at[group_no, hop]).wait()

    def for_origins(hop, item):
        if hop == 0:
            item(y)
        elif hop == half:
            item(origin_of(0, hop))
        else:

            def both(way, carry):
                item(lax.rem(y + ny + (2 * way - 1) * hop, ny))
                return carry

            lax.fori_loop(0, 2, both, 0)

    def mix_item(g, first):
        at = mix.group(g)

        def item(origin):
            a = jnp.concatenate([pg[origin, 0, at, :], pg[origin, 1, at, :]], axis=1)
            rows = pl.ds(pl.multiple_of(origin * 2 * chans, 2 * chans), 2 * chans)
            got = jnp.dot(a, mw[rows, :], preferred_element_type=jnp.float32)
            acc_m[at, :] = got if first else acc_m[at, :] + got

        return item

    def token_item(ch, first):
        at = tok.group(ch)

        def item(origin):
            scaled, sums = [], 0.0
            for j in range(2):
                x = tg[origin, j, at, :].astype(jnp.float32)
                lanes = pl.ds(pl.multiple_of((origin * 2 + j) * feats, feats), feats)
                scaled.append((x * gain_in[:, lanes]).astype(jnp.bfloat16))
                sq = x * x
                for q in range(0, feats, 128):
                    sums = sums + sq[:, q : q + 128]
            rows = pl.ds(pl.multiple_of(origin * 2 * feats, 2 * feats), 2 * feats)
            got = jnp.dot(
                jnp.concatenate(scaled, axis=1), wgu[rows, :], preferred_element_type=jnp.float32
            )
            if first:
                acc_t[at, :] = got
                squares[at, :] = sums
            else:
                acc_t[at, :] = acc_t[at, :] + got
                squares[at, :] = squares[at, :] + sums

        return item

    def down_item(ch, first):
        at = tok.group(ch)

        def item(origin):
            a = jnp.concatenate([hg[origin, 0, at, :], hg[origin, 1, at, :]], axis=1)
            rows = pl.ds(pl.multiple_of(origin * 2 * hid, 2 * hid), 2 * hid)
            got = jnp.dot(a, wd[rows, :], preferred_element_type=jnp.float32)
            acc_d[at, :] = got if first else acc_d[at, :] + got

        return item

    def activate(ch):
        at = tok.group(ch)
        total = jnp.sum(squares[at, :], axis=1, keepdims=True)
        inverse = lax.rsqrt(total / (feats * tp_size) + EPS)
        gate = acc_t[at, pl.ds(0, hid)] * inverse
        upper = acc_t[at, pl.ds(hid, hid)] * inverse
        hg[y, core, at, :] = (gate / (1.0 + jnp.exp(-gate)) * upper).astype(jnp.bfloat16)

    def inside(device, ch):
        return jnp.logical_and(device >= bounds[ch], device < bounds[ch + 1])

    def dispatched(ch):
        base, rows = tok.group_first[ch], chunks[ch]
        mine = inside(ep, ch)

        @pl.when(mine)
        def _():
            if rows > cap:
                ref = tg.at[0, 0, pl.ds(base, rows - cap), :]
                pltpu.make_async_copy(ref, ref, disp_recv.at[ch]).wait()
            tg[y, core, block(ep), :] = outgoing[block(ep), :]

        @pl.when(jnp.logical_not(mine))
        def _():
            ref = tg.at[0, 0, pl.ds(base, rows), :]
            pltpu.make_async_copy(ref, ref, disp_recv.at[ch]).wait()

    def give_back(ch):
        at = tok.group(ch)
        produced[at, :] = acc_d[at, :].astype(jnp.bfloat16)

        def one(i, carry):
            other = bounds[ch] + lax.rem(ep + i, sources[ch])

            @pl.when(other != ep)
            def _():
                pltpu.make_async_remote_copy(
                    src_ref=produced.at[block(other), :],
                    dst_ref=returned.at[block(ep), :],
                    send_sem=ret_send,
                    recv_sem=ret_recv,
                    device_id=(other, tp),
                    device_id_type=MESH,
                ).start()

            return carry

        lax.fori_loop(0, sources[ch], one, 0)

        @pl.when(inside(ep, ch))
        def _():
            returned[block(ep), :] = produced[block(ep), :]

    def first_rows():
        halo_copy.wait_recv()
        ext[pl.ds(0, REACH), :] = jnp.where(ep == 0, 0.0, halo[...].astype(jnp.float32))
        position = ep * length + lax.broadcasted_iota(jnp.int32, (REACH, chans), 0)
        counts = jnp.minimum(position + 1, window).astype(jnp.float32)
        pg[y, core, pl.ds(0, REACH), :] = (
            window_sum(0, REACH) / counts - ext[pl.ds(REACH, REACH), :]
        ).astype(jnp.bfloat16)

    streams = {"m": mix, "t": tok, "h": hdn}
    weights = {"mc": [0], "tc": [1, 2], "hc": [3]}
    for entry in order:
        kind = entry[0]
        for i in weights.pop(kind, ()):
            w_copies[i].wait()
        if kind in streams:
            move(streams[kind], entry[1], entry[2])
        elif kind == "disp":
            lax.fori_loop(1, ep_size, dispatch, 0)
        elif kind == "pool":
            pool(entry[1])
        elif kind == "first":
            first_rows()
        elif kind == "got":
            dispatched(entry[1])
        elif kind == "mc":
            mate_wait(mix, entry[1], entry[2])
            for_origins(entry[2], mix_item(entry[1], entry[2] == 0))
        elif kind == "mo":
            mixed_out[...] = acc_m[...].astype(jnp.bfloat16)
        elif kind == "tc":
            mate_wait(tok, entry[1], entry[2])
            for_origins(entry[2], token_item(entry[1], entry[2] == 0))
        elif kind == "act":
            activate(entry[1])
        elif kind == "hc":
            mate_wait(hdn, entry[1], entry[2])
            for_origins(entry[2], down_item(entry[1], entry[2] == 0))
        elif kind == "ret":
            give_back(entry[1])

    halo_copy.wait_send()
    others = pl.ds(0, slots - cap)
    pltpu.make_async_copy(outgoing.at[others, :], outgoing.at[others, :], disp_send).wait()
    pltpu.make_async_copy(produced.at[others, :], produced.at[others, :], ret_send).wait()
    for stream in streams.values():
        for piece in range(2 * len(stream.group_rows)):
            ref = stream.buf.at[pl.ds(0, ny - 1), 0, pl.ds(*stream.rows(piece)), :]
            pltpu.make_async_copy(ref, ref, stream.send.at[piece]).wait()
            ref = stream.buf.at[pl.ds(0, ny), 0, pl.ds(*stream.rows(piece)), :]
            pltpu.make_async_copy(ref, ref, stream.mate_send.at[piece]).wait()

    slot_lanes = lax.broadcasted_iota(jnp.int32, (tokens, slots), 1)
    takes = [
        (columns[:, k : k + 1].astype(jnp.int32) == slot_lanes).astype(jnp.bfloat16)
        for k in range(TOP)
    ]
    pltpu.make_async_copy(returned.at[others, :], returned.at[others, :], ret_recv).wait()
    rows = 0.0
    for k in range(TOP):
        picked = jnp.dot(takes[k], returned[...], preferred_element_type=jnp.float32)
        rows = rows + picked * columns[:, TOP + k : TOP + k + 1]
    rows_out[...] = rows.astype(jnp.bfloat16)


SOURCES = (12, 12, 8)
ORDER = (
    ("disp",), ("pool", 2), ("pool", 1), ("pool", 3), ("m", 1, 0), ("m", 3, 0), ("m", 2, 0),
    ("pool", 0), ("first",), ("m", 0, 0), ("m", 1, 1), ("mc", 1, 0), ("m", 3, 1), ("m", 2, 1),
    ("got", 0), ("t", 0, 0), ("m", 0, 1), ("got", 1), ("m", 1, 2), ("m", 3, 2), ("m", 2, 2),
    ("t", 0, 1), ("m", 0, 2), ("t", 3, 0), ("got", 2), ("t", 5, 0), ("m", 3, 3), ("mc", 1, 1),
    ("m", 2, 3), ("mc", 0, 0), ("t", 1, 0), ("t", 0, 2), ("t", 2, 0), ("tc", 0, 0), ("t", 4, 0),
    ("t", 5, 1), ("t", 1, 1), ("m", 0, 3), ("tc", 2, 0), ("tc", 1, 0), ("mc", 1, 3), ("m", 3, 4),
    ("mc", 0, 2), ("m", 2, 4), ("m", 1, 3), ("t", 2, 1), ("t", 3, 1), ("t", 4, 1), ("t", 1, 2),
    ("mc", 0, 1), ("mc", 1, 4), ("m", 0, 4), ("tc", 0, 1), ("tc", 1, 1), ("t", 2, 2), ("t", 3, 2),
    ("mc", 0, 3), ("t", 5, 2), ("t", 0, 3), ("t", 1, 3), ("t", 4, 2), ("m", 1, 4), ("mc", 0, 4),
    ("t", 3, 3), ("t", 2, 3), ("tc", 0, 2), ("tc", 0, 3), ("tc", 2, 1), ("tc", 1, 2), ("t", 5, 3),
    ("t", 1, 4), ("t", 0, 4), ("mc", 1, 2), ("t", 4, 3), ("tc", 1, 3), ("tc", 0, 4), ("act", 0),
    ("h", 0, 0), ("h", 1, 0), ("t", 3, 4), ("t", 2, 4), ("t", 5, 4), ("tc", 2, 2), ("tc", 1, 4),
    ("act", 1), ("h", 2, 0), ("t", 4, 4), ("tc", 2, 3), ("h", 3, 0), ("hc", 0, 0), ("h", 0, 1),
    ("tc", 2, 4), ("act", 2), ("h", 4, 0), ("h", 5, 0), ("hc", 1, 0), ("h", 1, 1), ("h", 2, 1),
    ("hc", 0, 1), ("h", 3, 1), ("h", 0, 2), ("h", 4, 1), ("h", 5, 1), ("h", 1, 2), ("h", 2, 2),
    ("mo",), ("h", 3, 2), ("h", 4, 2), ("h", 5, 2), ("h", 0, 3), ("hc", 1, 1), ("hc", 2, 0),
    ("h", 1, 3), ("h", 2, 3), ("hc", 1, 2), ("h", 3, 3), ("h", 4, 3), ("h", 5, 3), ("hc", 0, 2),
    ("hc", 2, 2), ("hc", 2, 1), ("h", 1, 4), ("h", 0, 4), ("hc", 0, 3), ("hc", 1, 3), ("h", 2, 4),
    ("h", 3, 4), ("hc", 0, 4), ("ret", 0), ("h", 4, 4), ("h", 5, 4), ("hc", 2, 3), ("hc", 1, 4),
    ("ret", 1), ("hc", 2, 4), ("ret", 2),
)


def full_order(ep_size, half):
    sources = SOURCES if ep_size == sum(SOURCES) else (1, ep_size - 2, 1)
    if half == 4:
        return sources, ORDER
    order = [("disp",), ("pool", 1), ("pool", 2), ("pool", 3), ("pool", 0), ("first",)]
    for kind, groups in (("m", MIX_GROUPS), ("t", 3), ("h", 3)):
        for g in range(groups):
            order += [("got", g)] if kind == "t" else []
            order += [(kind, 2 * g + q, hop) for hop in range(half + 1) for q in range(2)]
            order += [(kind + "c", g, hop) for hop in range(half + 1)]
            order += {"m": [("mo",)] * (g == 1), "t": [("act", g)], "h": [("ret", g)]}[kind]
    return sources, order


def solution(mesh):
    ep_size, tp_size = mesh.shape["ep"], mesh.shape["tp"]
    ny = tp_size // 2
    half = ny // 2

    def shards(mix_input, mix_weight, expert_input, expert_index, route_share, norm_gain, gate_weight, up_weight, down_weight):
        length, chans = mix_input.shape
        tokens, feats = expert_input.shape
        slots = 2 * tokens * TOP
        width = mix_weight.shape[1]
        hid = gate_weight.shape[2]
        vmem, dma = pltpu.VMEM, pltpu.SemaphoreType.DMA
        bf16, f32 = jnp.bfloat16, jnp.float32

        sources, order = full_order(ep_size, half)
        chunks = len(sources)

        def stream_sems(groups):
            pieces = 2 * groups
            return [dma((pieces,)), dma((pieces, 2, half)), dma((pieces,)), dma((groups, half + 1))]

        here = pl.BlockSpec(memory_space=pltpu.VMEM)
        there = pl.BlockSpec(memory_space=pltpu.HBM)
        flops = 2 * (length * chans * tp_size * width + slots * (feats * tp_size * 2 * hid + hid * tp_size * width))
        call = pl.pallas_call(
            functools.partial(
                kernel, ep_size, tp_size, chans * tp_size // 4, sources, order
            ),
            name="mixer_and_experts",
            out_shape=(
                jax.ShapeDtypeStruct((length, width), bf16),
                jax.ShapeDtypeStruct((tokens, width), bf16),
            ),
            in_specs=[there] * 9,
            out_specs=(here, here),
            scratch_shapes=[
                vmem((length, chans), bf16),
                vmem((tokens, feats), bf16),
                vmem((TOP, tokens), jnp.int32),
                vmem((TOP, tokens), f32),
                vmem((1, feats * tp_size), f32),
                vmem(mix_weight.shape, bf16),
                vmem((feats * tp_size, 2 * hid), bf16),
                vmem(down_weight.shape[1:], bf16),
                vmem((length + REACH, chans), f32),
                vmem((REACH, chans), bf16),
                vmem((ny, 2, length, chans), bf16),
                vmem((ny, 2, slots, feats), bf16),
                vmem((ny, 2, slots, hid), bf16),
                vmem((slots, feats), bf16),
                vmem((slots, width), bf16),
                vmem((slots, width), bf16),
                vmem((length, width), f32),
                vmem((slots, 2 * hid), f32),
                vmem((slots, width), f32),
                vmem((slots, 128), f32),
                vmem((tokens, tokens), f32),
                dma((5,)),
                dma((4,)),
                dma((2,)),
                dma,
                dma((chunks,)),
                dma,
                dma,
            ]
            + stream_sems(MIX_GROUPS)
            + stream_sems(chunks)
            + stream_sems(chunks),
            compiler_params=pltpu.CompilerParams(
                collective_id=0, has_side_effects=True, vmem_limit_bytes=24 * 1024 * 1024
            ),
            cost_estimate=pl.CostEstimate(flops=flops, bytes_accessed=8 * 1024 * 1024, transcendentals=0),
        )
        operands = (
            mix_input,
            expert_input,
            expert_index.T,
            route_share.T,
            norm_gain.reshape(1, -1),
            mix_weight,
            gate_weight[0],
            up_weight[0],
            down_weight[0],
        )
        return call(*(pltpu.with_memory_space_constraint(a, pltpu.HBM) for a in operands))

    placed = (
        P("ep", "tp"),
        P(None, "tp"),
        P("ep", "tp"),
        P("ep", None),
        P("ep", None),
        P(),
        P("ep", None, "tp"),
        P("ep", None, "tp"),
        P("ep", None, "tp"),
    )
    return jax.shard_map(
        shards,
        mesh=mesh,
        in_specs=placed,
        out_specs=(P("ep", "tp"), P("ep", "tp")),
        check_vma=False,
    )
```

```python
import functools

import jax
import jax.numpy as jnp
from jax import lax
from jax.experimental import pallas as pl
from jax.experimental.pallas import tpu as pltpu
from jax.sharding import PartitionSpec as P

MESH = pl.DeviceIdType.MESH
TOP = 2
REACH = 16
EPS = 1e-06
MIX_GROUPS = 2
PARTS = ((0, 1), (2, 3), (4,))
NX = 4


class Stream:
    def __init__(self, buf, group_rows, sems):
        self.buf = buf
        self.group_rows = group_rows
        self.group_first = [sum(group_rows[:g]) for g in range(len(group_rows))]
        self.send, self.recv, self.mate_send, self.mate_recv = sems

    def group(self, g):
        return pl.ds(self.group_first[g], self.group_rows[g])

    def rows(self, piece):
        size = self.group_rows[piece // 2] // 2
        return self.group_first[piece // 2] + (piece % 2) * size, size


def far_first(nz, nx):
    def hops(offset):
        return min(offset[0], nz - offset[0]) + min(offset[1], nx - offset[1])

    offsets = [(z, x) for z in range(nz) for x in range(nx) if z or x]
    return sorted(offsets, key=lambda offset: (-hops(offset), offset))


def kernel(
    ep_size,
    tp_size,
    group_size,
    sources,
    order,
    mix_hbm,
    x_hbm,
    index_hbm,
    share_hbm,
    gain_hbm,
    mix_w,
    gate_w,
    up_w,
    down_w,
    mixed_out,
    rows_out,
    mix_in,
    x_in,
    index_in,
    share_in,
    gain_in,
    mw,
    wgu,
    wd,
    ext,
    halo,
    pg,
    tg,
    hg,
    outgoing,
    produced,
    returned,
    acc_m,
    acc_t,
    acc_d,
    squares,
    columns,
    takes,
    in_sem,
    w_sem,
    halo_sem,
    disp_send,
    disp_recv,
    ret_send,
    ret_recv,
    m_send,
    m_recv,
    m_mate_send,
    m_mate_recv,
    t_send,
    t_recv,
    t_mate_send,
    t_mate_recv,
    h_send,
    h_recv,
    h_mate_send,
    h_mate_recv,
):
    ep = lax.axis_index("ep")
    tp = lax.axis_index("tp")
    ny = tp_size // 2
    half = ny // 2
    core = lax.rem(tp, 2)
    y = tp // 2
    up = lax.rem(tp + 2, tp_size)
    down = lax.rem(tp + tp_size - 2, tp_size)
    mate = tp + 1 - 2 * core
    tokens, feats = x_in.shape
    length, chans = mix_in.shape
    slots = outgoing.shape[0]
    cap = slots // ep_size
    nx = NX if ep_size % NX == 0 else 1
    hid = hg.shape[3]
    chunks = [n * cap for n in sources]
    bounds = [sum(sources[:ch]) for ch in range(len(sources) + 1)]

    mix = Stream(pg, [length // MIX_GROUPS] * MIX_GROUPS, (m_send, m_recv, m_mate_send, m_mate_recv))
    tok = Stream(tg, chunks, (t_send, t_recv, t_mate_send, t_mate_recv))
    hdn = Stream(hg, chunks, (h_send, h_recv, h_mate_send, h_mate_recv))

    def block(i):
        return pl.ds(pl.multiple_of(i * cap, cap), cap)

    in_copies = [
        pltpu.make_async_copy(src, dst, in_sem.at[i])
        for i, (src, dst) in enumerate(
            (
                (index_hbm, index_in),
                (x_hbm, x_in),
                (share_hbm, share_in),
                (mix_hbm, mix_in),
                (gain_hbm, gain_in),
            )
        )
    ]
    for copy in in_copies:
        copy.start()
    w_copies = [
        pltpu.make_async_copy(mix_w, mw, w_sem.at[0]),
        pltpu.make_async_copy(gate_w, wgu.at[:, pl.ds(0, hid)], w_sem.at[1]),
        pltpu.make_async_copy(up_w, wgu.at[:, pl.ds(hid, hid)], w_sem.at[2]),
        pltpu.make_async_copy(down_w, wd, w_sem.at[3]),
    ]
    for copy in w_copies:
        copy.start()

    barrier = pltpu.get_barrier_semaphore()
    for other in (up, down, mate):
        pl.semaphore_signal(barrier, inc=1, device_id=(ep, other), device_id_type=MESH)

    def greet(i, carry):
        pl.semaphore_signal(
            barrier, inc=1, device_id=(lax.rem(ep + i, ep_size), tp), device_id_type=MESH
        )
        return carry

    lax.fori_loop(1, ep_size, greet, 0)

    for copy in in_copies:
        copy.wait()

    expert_rows = lax.broadcasted_iota(jnp.int32, (ep_size, tokens), 0)
    named = [index_in[k : k + 1, :] for k in range(TOP)]
    hits = [(expert_rows == named[k]).astype(jnp.float32) for k in range(TOP)]
    before = (
        lax.broadcasted_iota(jnp.int32, (tokens, tokens), 0)
        < lax.broadcasted_iota(jnp.int32, (tokens, tokens), 1)
    ).astype(jnp.bfloat16)
    earlier = jnp.dot(
        (hits[0] + hits[1]).astype(jnp.bfloat16), before, preferred_element_type=jnp.float32
    )
    ranks = [
        jnp.sum(earlier * hits[0], axis=0, keepdims=True),
        jnp.sum((earlier + hits[0]) * hits[1], axis=0, keepdims=True),
    ]
    targets = [named[k] * cap + ranks[k].astype(jnp.int32) for k in range(TOP)]
    slot_rows = lax.broadcasted_iota(jnp.int32, (slots, tokens), 0)
    picks = jnp.logical_or(slot_rows == targets[0], slot_rows == targets[1])
    outgoing[...] = jnp.dot(
        picks.astype(jnp.bfloat16), x_in[...], preferred_element_type=jnp.float32
    ).astype(jnp.bfloat16)
    total_share = share_in[0:1, :] + share_in[1:2, :]
    row_id = lax.broadcasted_iota(jnp.int32, (tokens, tokens), 0)
    packed = jnp.zeros((tokens, tokens), jnp.float32)
    packed = jnp.where(row_id == 0, targets[0].astype(jnp.float32), packed)
    packed = jnp.where(row_id == 1, targets[1].astype(jnp.float32), packed)
    packed = jnp.where(row_id == 2, share_in[0:1, :] / total_share, packed)
    packed = jnp.where(row_id == 3, share_in[1:2, :] / total_share, packed)
    columns[...] = packed.T

    ext[pl.ds(REACH, length), :] = mix_in[...].astype(jnp.float32)
    group = (tp * chans) // group_size
    window = jnp.where(group == 0, 2, jnp.where(group == 1, 4, jnp.where(group == 2, 8, 16)))

    def window_sum(first, count):
        running = ext[pl.ds(REACH + first, count), :]
        for lag in range(1, REACH):
            running = running + jnp.where(
                lag < window, ext[pl.ds(REACH + first - lag, count), :], 0.0
            )
        return running

    inverse_window = jnp.where(
        group == 0, 0.5, jnp.where(group == 1, 0.25, jnp.where(group == 2, 0.125, 0.0625))
    )
    def pool(piece):
        at, size = mix.rows(piece)
        for first in range(at, at + size, min(64, size)):
            skip = REACH if first == 0 else 0
            begin, count = first + skip, min(64, size) - skip
            if count:
                pg[y, core, pl.ds(begin, count), :] = (
                    window_sum(begin, count) * inverse_window - ext[pl.ds(REACH + begin, count), :]
                ).astype(jnp.bfloat16)

    pl.semaphore_wait(barrier, ep_size - 1 + 3)

    halo_copy = pltpu.make_async_remote_copy(
        src_ref=mix_in.at[pl.ds(length - REACH, REACH), :],
        dst_ref=halo,
        send_sem=halo_sem.at[0],
        recv_sem=halo_sem.at[1],
        device_id=(lax.rem(ep + 1, ep_size), tp),
        device_id_type=MESH,
    )
    halo_copy.start()

    my_chunk = 0
    for bound in bounds[1:-1]:
        my_chunk = my_chunk + jnp.where(ep >= bound, 1, 0)

    def dispatch():
        for away_z, away_x in far_first(ep_size // nx, nx):
            other = lax.rem(ep // nx + away_z, ep_size // nx) * nx + lax.rem(ep + away_x, nx)
            pltpu.make_async_remote_copy(
                src_ref=outgoing.at[block(other), :],
                dst_ref=tg.at[y, core, block(ep), :],
                send_sem=disp_send,
                recv_sem=disp_recv.at[my_chunk],
                device_id=(other, tp),
                device_id_type=MESH,
            ).start()

    def limit(piece, way):
        return half if (piece % 2 == 0) == (way == 0) else half - 1

    def arrival(piece, way, hop):
        return piece * (ny - 1) + way * limit(piece, 0) + hop - 1

    def part_of(hop):
        return [hop in hops for hops in PARTS].index(True)

    def part(stream, origin, piece):
        return stream.buf.at[origin, core, pl.ds(*stream.rows(piece)), :]

    def ring_send(stream, piece, way, origin, hop):
        ref = part(stream, origin, piece)
        pltpu.make_async_remote_copy(
            src_ref=ref,
            dst_ref=ref,
            send_sem=stream.send,
            recv_sem=stream.recv.at[arrival(piece, way, hop + 1)],
            device_id=(ep, up if way == 0 else down),
            device_id_type=MESH,
        ).start()

    def mate_copy(stream, piece, origin, hop):
        ref = part(stream, origin, piece)
        pltpu.make_async_remote_copy(
            src_ref=ref,
            dst_ref=ref,
            send_sem=stream.mate_send,
            recv_sem=stream.mate_recv.at[piece // 2, part_of(hop)],
            device_id=(ep, mate),
            device_id_type=MESH,
        ).start()

    def origin_of(way, hop):
        return lax.rem(y + ny - hop, ny) if way == 0 else lax.rem(y + hop, ny)

    def move(stream, piece, hop):
        if hop == 0:
            for way in range(2):
                if limit(piece, way) > 0:
                    ring_send(stream, piece, way, y, 0)
            mate_copy(stream, piece, y, 0)
            return
        for way in range(2):
            if hop > limit(piece, way):
                continue
            origin = origin_of(way, hop)
            ref = part(stream, origin, piece)
            pltpu.make_async_copy(ref, ref, stream.recv.at[arrival(piece, way, hop)]).wait()
            if hop < limit(piece, way):
                ring_send(stream, piece, way, origin, hop)
            mate_copy(stream, piece, origin, hop)

    def mate_wait(stream, group_no, part_no):
        origins = sum(1 if hop in (0, half) else 2 for hop in PARTS[part_no])
        ref = stream.buf.at[pl.ds(0, origins), 0, stream.group(group_no), :]
        pltpu.make_async_copy(ref, ref, stream.mate_recv.at[group_no, part_no]).wait()

    def gathered(stream, group_no, part_no, item_of):
        mate_wait(stream, group_no, part_no)
        for hop in PARTS[part_no]:
            for_origins(hop, item_of(group_no, hop == 0))

    def for_origins(hop, item):
        if hop == 0:
            item(y)
        elif hop == half:
            item(origin_of(0, hop))
        else:

            def both(way, carry):
                item(lax.rem(y + ny + (2 * way - 1) * hop, ny))
                return carry

            lax.fori_loop(0, 2, both, 0)

    def mix_item(g, first):
        at = mix.group(g)

        def item(origin):
            a = jnp.concatenate([pg[origin, 0, at, :], pg[origin, 1, at, :]], axis=1)
            rows = pl.ds(pl.multiple_of(origin * 2 * chans, 2 * chans), 2 * chans)
            got = jnp.dot(a, mw[rows, :], preferred_element_type=jnp.float32)
            acc_m[at, :] = got if first else acc_m[at, :] + got

        return item

    def token_item(ch, first):
        at = tok.group(ch)

        def item(origin):
            scaled, sums = [], 0.0
            for j in range(2):
                x = tg[origin, j, at, :].astype(jnp.float32)
                lanes = pl.ds(pl.multiple_of((origin * 2 + j) * feats, feats), feats)
                scaled.append((x * gain_in[:, lanes]).astype(jnp.bfloat16))
                sq = x * x
                for q in range(0, feats, 128):
                    sums = sums + sq[:, q : q + 128]
            rows = pl.ds(pl.multiple_of(origin * 2 * feats, 2 * feats), 2 * feats)
            got = jnp.dot(
                jnp.concatenate(scaled, axis=1), wgu[rows, :], preferred_element_type=jnp.float32
            )
            if first:
                acc_t[at, :] = got
                squares[at, :] = sums
            else:
                acc_t[at, :] = acc_t[at, :] + got
                squares[at, :] = squares[at, :] + sums

        return item

    def down_item(ch, first):
        at = tok.group(ch)

        def item(origin):
            a = jnp.concatenate([hg[origin, 0, at, :], hg[origin, 1, at, :]], axis=1)
            rows = pl.ds(pl.multiple_of(origin * 2 * hid, 2 * hid), 2 * hid)
            got = jnp.dot(a, wd[rows, :], preferred_element_type=jnp.float32)
            acc_d[at, :] = got if first else acc_d[at, :] + got

        return item

    def activate(ch):
        at = tok.group(ch)
        total = jnp.sum(squares[at, :], axis=1, keepdims=True)
        inverse = lax.rsqrt(total / (feats * tp_size) + EPS)
        gate = acc_t[at, pl.ds(0, hid)] * inverse
        upper = acc_t[at, pl.ds(hid, hid)] * inverse
        hg[y, core, at, :] = (gate / (1.0 + jnp.exp(-gate)) * upper).astype(jnp.bfloat16)

    def inside(device, ch):
        return jnp.logical_and(device >= bounds[ch], device < bounds[ch + 1])

    def dispatched(ch):
        base, rows = tok.group_first[ch], chunks[ch]
        mine = inside(ep, ch)

        @pl.when(mine)
        def _():
            if rows > cap:
                ref = tg.at[0, 0, pl.ds(base, rows - cap), :]
                pltpu.make_async_copy(ref, ref, disp_recv.at[ch]).wait()
            tg[y, core, block(ep), :] = outgoing[block(ep), :]

        @pl.when(jnp.logical_not(mine))
        def _():
            ref = tg.at[0, 0, pl.ds(base, rows), :]
            pltpu.make_async_copy(ref, ref, disp_recv.at[ch]).wait()

    def give_back(ch):
        at = tok.group(ch)
        produced[at, :] = acc_d[at, :].astype(jnp.bfloat16)

        def one(i, carry):
            other = bounds[ch] + lax.rem(ep + i, sources[ch])

            @pl.when(other != ep)
            def _():
                pltpu.make_async_remote_copy(
                    src_ref=produced.at[block(other), :],
                    dst_ref=returned.at[block(ep), :],
                    send_sem=ret_send,
                    recv_sem=ret_recv,
                    device_id=(other, tp),
                    device_id_type=MESH,
                ).start()

            return carry

        lax.fori_loop(0, sources[ch], one, 0)

        @pl.when(inside(ep, ch))
        def _():
            returned[block(ep), :] = produced[block(ep), :]

    def find_takes():
        slot_lanes = lax.broadcasted_iota(jnp.int32, (tokens, slots), 1)
        for k in range(TOP):
            takes[k] = (columns[:, k : k + 1].astype(jnp.int32) == slot_lanes).astype(jnp.bfloat16)

    def first_rows():
        halo_copy.wait_recv()
        ext[pl.ds(0, REACH), :] = jnp.where(ep == 0, 0.0, halo[...].astype(jnp.float32))
        position = ep * length + lax.broadcasted_iota(jnp.int32, (REACH, chans), 0)
        counts = jnp.minimum(position + 1, window).astype(jnp.float32)
        pg[y, core, pl.ds(0, REACH), :] = (
            window_sum(0, REACH) / counts - ext[pl.ds(REACH, REACH), :]
        ).astype(jnp.bfloat16)

    streams = {"m": mix, "t": tok, "h": hdn}
    weights = {"mc": [0], "tc": [1, 2], "hc": [3]}
    for entry in order:
        kind = entry[0]
        for i in weights.pop(kind, ()):
            w_copies[i].wait()
        if kind in streams:
            move(streams[kind], entry[1], entry[2])
        elif kind == "disp":
            dispatch()
        elif kind == "take":
            find_takes()
        elif kind == "pool":
            pool(entry[1])
        elif kind == "first":
            first_rows()
        elif kind == "got":
            dispatched(entry[1])
        elif kind == "mc":
            gathered(mix, entry[1], entry[2], mix_item)
        elif kind == "mo":
            mixed_out[...] = acc_m[...].astype(jnp.bfloat16)
        elif kind == "tc":
            gathered(tok, entry[1], entry[2], token_item)
        elif kind == "act":
            activate(entry[1])
        elif kind == "hc":
            gathered(hdn, entry[1], entry[2], down_item)
        elif kind == "ret":
            give_back(entry[1])

    halo_copy.wait_send()
    others = pl.ds(0, slots - cap)
    pltpu.make_async_copy(outgoing.at[others, :], outgoing.at[others, :], disp_send).wait()
    pltpu.make_async_copy(produced.at[others, :], produced.at[others, :], ret_send).wait()
    for stream in streams.values():
        ref = stream.buf.at[pl.ds(0, ny - 1), 0, :, :]
        pltpu.make_async_copy(ref, ref, stream.send).wait()
        ref = stream.buf.at[:, 0, :, :]
        pltpu.make_async_copy(ref, ref, stream.mate_send).wait()

    pltpu.make_async_copy(returned.at[others, :], returned.at[others, :], ret_recv).wait()
    rows = 0.0
    for k in range(TOP):
        picked = jnp.dot(takes[k], returned[...], preferred_element_type=jnp.float32)
        rows = rows + picked * columns[:, TOP + k : TOP + k + 1]
    rows_out[...] = rows.astype(jnp.bfloat16)


SOURCES = (8, 8, 8, 8)
ORDER = (
    ("disp",), ("pool", 1), ("pool", 2), ("pool", 3), ("m", 1, 0), ("m", 2, 0), ("m", 2, 1),
    ("take",), ("got", 1), ("got", 3), ("got", 2), ("t", 7, 0), ("got", 0), ("t", 0, 0),
    ("t", 1, 0), ("t", 6, 0), ("t", 3, 0), ("t", 5, 0), ("t", 4, 0), ("t", 2, 0), ("t", 0, 1),
    ("t", 1, 1), ("pool", 0), ("first",), ("t", 3, 1), ("t", 5, 1), ("t", 7, 1), ("t", 2, 1),
    ("t", 4, 1), ("t", 0, 2), ("t", 1, 2), ("t", 6, 1), ("t", 3, 2), ("tc", 3, 0), ("t", 2, 2),
    ("t", 5, 2), ("t", 4, 2), ("t", 1, 3), ("tc", 1, 0), ("t", 0, 3), ("tc", 0, 0), ("t", 6, 2),
    ("t", 7, 2), ("t", 3, 3), ("t", 2, 3), ("t", 5, 3), ("m", 3, 0), ("t", 4, 3), ("m", 1, 1),
    ("t", 1, 4), ("t", 0, 4), ("tc", 0, 1), ("t", 6, 3), ("tc", 2, 0), ("t", 7, 3), ("tc", 0, 2),
    ("act", 0), ("h", 0, 0), ("m", 0, 0), ("h", 1, 0), ("t", 3, 4), ("t", 2, 4), ("tc", 1, 1),
    ("t", 5, 4), ("m", 2, 2), ("tc", 3, 1), ("tc", 1, 2), ("t", 4, 4), ("act", 1), ("h", 2, 0),
    ("m", 1, 2), ("h", 3, 0), ("tc", 2, 1), ("t", 7, 4), ("t", 6, 4), ("h", 0, 1), ("tc", 2, 2),
    ("act", 2), ("h", 5, 0), ("h", 4, 0), ("h", 1, 1), ("tc", 3, 2), ("act", 3), ("h", 7, 0),
    ("h", 6, 0), ("h", 2, 1), ("m", 3, 1), ("h", 0, 2), ("h", 5, 1), ("h", 4, 1), ("h", 3, 1),
    ("h", 1, 2), ("h", 7, 1), ("h", 6, 1), ("h", 2, 2), ("hc", 0, 0), ("hc", 1, 0), ("m", 0, 1),
    ("hc", 2, 0), ("h", 5, 2), ("h", 4, 2), ("h", 3, 2), ("h", 0, 3), ("h", 1, 3), ("h", 7, 2),
    ("h", 6, 2), ("h", 2, 3), ("m", 3, 2), ("mc", 1, 0), ("hc", 0, 1), ("h", 5, 3), ("h", 4, 3),
    ("m", 0, 2), ("h", 3, 3), ("h", 1, 4), ("h", 7, 3), ("h", 0, 4), ("h", 6, 3), ("hc", 3, 0),
    ("hc", 2, 1), ("m", 2, 3), ("m", 1, 3), ("hc", 0, 2), ("ret", 0), ("h", 2, 4), ("h", 5, 4),
    ("h", 4, 4), ("m", 3, 3), ("hc", 1, 1), ("m", 0, 3), ("h", 3, 4), ("h", 7, 4), ("h", 6, 4),
    ("hc", 2, 2), ("ret", 2), ("hc", 3, 1), ("hc", 1, 2), ("ret", 1), ("m", 1, 4), ("hc", 3, 2),
    ("ret", 3), ("mc", 0, 0), ("mc", 1, 1), ("m", 2, 4), ("m", 0, 4), ("m", 3, 4), ("mc", 0, 1),
    ("mc", 0, 2), ("mc", 1, 2), ("mo",),
)


def solution(mesh):
    ep_size, tp_size = mesh.shape["ep"], mesh.shape["tp"]
    ny = tp_size // 2
    half = ny // 2

    def shards(mix_input, mix_weight, expert_input, expert_index, route_share, norm_gain, gate_weight, up_weight, down_weight):
        length, chans = mix_input.shape
        tokens, feats = expert_input.shape
        slots = 2 * tokens * TOP
        width = mix_weight.shape[1]
        hid = gate_weight.shape[2]
        vmem, dma = pltpu.VMEM, pltpu.SemaphoreType.DMA
        bf16, f32 = jnp.bfloat16, jnp.float32

        sources = SOURCES if ep_size == sum(SOURCES) else (ep_size // len(SOURCES),) * len(SOURCES)
        chunks = len(sources)

        def stream_sems(groups):
            return [dma, dma((2 * groups * (ny - 1),)), dma, dma((groups, len(PARTS)))]

        here = pl.BlockSpec(memory_space=pltpu.VMEM)
        there = pl.BlockSpec(memory_space=pltpu.HBM)
        flops = 2 * (length * chans * tp_size * width + slots * (feats * tp_size * 2 * hid + hid * tp_size * width))
        call = pl.pallas_call(
            functools.partial(
                kernel, ep_size, tp_size, chans * tp_size // 4, sources, ORDER
            ),
            name="mixer_and_experts",
            out_shape=(
                jax.ShapeDtypeStruct((length, width), bf16),
                jax.ShapeDtypeStruct((tokens, width), bf16),
            ),
            in_specs=[there] * 9,
            out_specs=(here, here),
            scratch_shapes=[
                vmem((length, chans), bf16),
                vmem((tokens, feats), bf16),
                vmem((TOP, tokens), jnp.int32),
                vmem((TOP, tokens), f32),
                vmem((1, feats * tp_size), f32),
                vmem(mix_weight.shape, bf16),
                vmem((feats * tp_size, 2 * hid), bf16),
                vmem(down_weight.shape[1:], bf16),
                vmem((length + REACH, chans), f32),
                vmem((REACH, chans), bf16),
                vmem((ny, 2, length, chans), bf16),
                vmem((ny, 2, slots, feats), bf16),
                vmem((ny, 2, slots, hid), bf16),
                vmem((slots, feats), bf16),
                vmem((slots, width), bf16),
                vmem((slots, width), bf16),
                vmem((length, width), f32),
                vmem((slots, 2 * hid), f32),
                vmem((slots, width), f32),
                vmem((slots, 128), f32),
                vmem((tokens, tokens), f32),
                vmem((TOP, tokens, slots), bf16),
                dma((5,)),
                dma((4,)),
                dma((2,)),
                dma,
                dma((chunks,)),
                dma,
                dma,
            ]
            + stream_sems(MIX_GROUPS)
            + stream_sems(chunks)
            + stream_sems(chunks),
            compiler_params=pltpu.CompilerParams(
                collective_id=0, has_side_effects=True, vmem_limit_bytes=24 * 1024 * 1024
            ),
            cost_estimate=pl.CostEstimate(flops=flops, bytes_accessed=8 * 1024 * 1024, transcendentals=0),
        )
        operands = (
            mix_input,
            expert_input,
            expert_index.T,
            route_share.T,
            norm_gain.reshape(1, -1),
            mix_weight,
            gate_weight[0],
            up_weight[0],
            down_weight[0],
        )
        return call(*(pltpu.with_memory_space_constraint(a, pltpu.HBM) for a in operands))

    placed = (
        P("ep", "tp"),
        P(None, "tp"),
        P("ep", "tp"),
        P("ep", None),
        P("ep", None),
        P(),
        P("ep", None, "tp"),
        P("ep", None, "tp"),
        P("ep", None, "tp"),
    )
    return jax.shard_map(
        shards,
        mesh=mesh,
        in_specs=placed,
        out_specs=(P("ep", "tp"), P("ep", "tp")),
        check_vma=False,
    )
```

```python
import functools

import jax
import jax.numpy as jnp
from jax import lax
from jax.experimental import pallas as pl
from jax.experimental.pallas import tpu as pltpu
from jax.sharding import PartitionSpec as P

MESH = pl.DeviceIdType.MESH
TOP = 2
REACH = 16
EPS = 1e-06
MIX_GROUPS = 2
PARTS = ((0, 1), (2, 3), (4,))
NX = 4
HALVES = 1


class Stream:
    def __init__(self, buf, group_rows, sems):
        self.buf = buf
        self.group_rows = group_rows
        self.group_first = [sum(group_rows[:g]) for g in range(len(group_rows))]
        self.send, self.recv, self.mate_send, self.mate_recv = sems

    def group(self, g):
        return pl.ds(self.group_first[g], self.group_rows[g])

    def rows(self, piece):
        size = self.group_rows[piece // 2] // 2
        return self.group_first[piece // 2] + (piece % 2) * size, size


def far_first(nz, nx):
    def hops(offset):
        return min(offset[0], nz - offset[0]) + min(offset[1], nx - offset[1])

    offsets = [(z, x) for z in range(nz) for x in range(nx) if z or x]
    return sorted(offsets, key=lambda offset: (-hops(offset), offset))


def kernel(
    ep_size,
    tp_size,
    group_size,
    sources,
    order,
    mix_hbm,
    x_hbm,
    index_hbm,
    share_hbm,
    gain_hbm,
    mix_w,
    gate_w,
    up_w,
    down_w,
    mixed_out,
    rows_out,
    mix_in,
    x_in,
    index_in,
    share_in,
    gain_in,
    mw,
    wgu,
    wd,
    ext,
    halo,
    pg,
    tg,
    hg,
    outgoing,
    produced,
    returned,
    acc_m,
    acc_t,
    acc_d,
    squares,
    columns,
    takes,
    in_sem,
    w_sem,
    halo_sem,
    disp_send,
    disp_recv,
    ret_send,
    ret_recv,
    m_send,
    m_recv,
    m_mate_send,
    m_mate_recv,
    t_send,
    t_recv,
    t_mate_send,
    t_mate_recv,
    h_send,
    h_recv,
    h_mate_send,
    h_mate_recv,
):
    ep = lax.axis_index("ep")
    tp = lax.axis_index("tp")
    ny = tp_size // 2
    half = ny // 2
    core = lax.rem(tp, 2)
    y = tp // 2
    up = lax.rem(tp + 2, tp_size)
    down = lax.rem(tp + tp_size - 2, tp_size)
    mate = tp + 1 - 2 * core
    tokens, feats = x_in.shape
    length, chans = mix_in.shape
    slots = outgoing.shape[0]
    cap = slots // ep_size
    nx = NX if ep_size % NX == 0 else 1
    hid = hg.shape[3]
    part = cap // HALVES
    sets = len(sources)
    bounds = [sum(sources[:g]) for g in range(sets + 1)]
    chunks = [sources[ch // HALVES] * part for ch in range(sets * HALVES)]

    mix = Stream(pg, [length // MIX_GROUPS] * MIX_GROUPS, (m_send, m_recv, m_mate_send, m_mate_recv))
    tok = Stream(tg, chunks, (t_send, t_recv, t_mate_send, t_mate_recv))
    hdn = Stream(hg, chunks, (h_send, h_recv, h_mate_send, h_mate_recv))

    def sent_block(half_no, expert):
        return pl.ds(pl.multiple_of((half_no * ep_size + expert) * part, part), part)

    def chunk_block(ch, source):
        first = sum(chunks[:ch])
        return pl.ds(pl.multiple_of(first + (source - bounds[ch // HALVES]) * part, part), part)

    def my_block(half_no):
        first = (bounds[0] * HALVES + half_no * sources[0] + ep - bounds[0]) * part
        for g in range(1, sets):
            at = (bounds[g] * HALVES + half_no * sources[g] + ep - bounds[g]) * part
            first = jnp.where(ep >= bounds[g], at, first)
        return pl.ds(pl.multiple_of(first, part), part)

    in_copies = [
        pltpu.make_async_copy(src, dst, in_sem.at[i])
        for i, (src, dst) in enumerate(
            (
                (index_hbm, index_in),
                (x_hbm, x_in),
                (share_hbm, share_in),
                (mix_hbm, mix_in),
                (gain_hbm, gain_in),
            )
        )
    ]
    for copy in in_copies:
        copy.start()
    w_copies = [
        pltpu.make_async_copy(mix_w, mw, w_sem.at[0]),
        pltpu.make_async_copy(gate_w, wgu.at[:, pl.ds(0, hid)], w_sem.at[1]),
        pltpu.make_async_copy(up_w, wgu.at[:, pl.ds(hid, hid)], w_sem.at[2]),
        pltpu.make_async_copy(down_w, wd, w_sem.at[3]),
    ]
    for copy in w_copies:
        copy.start()

    barrier = pltpu.get_barrier_semaphore()
    for other in (up, down, mate):
        pl.semaphore_signal(barrier, inc=1, device_id=(ep, other), device_id_type=MESH)

    def greet(i, carry):
        pl.semaphore_signal(
            barrier, inc=1, device_id=(lax.rem(ep + i, ep_size), tp), device_id_type=MESH
        )
        return carry

    lax.fori_loop(1, ep_size, greet, 0)

    for copy in in_copies:
        copy.wait()

    expert_rows = lax.broadcasted_iota(jnp.int32, (ep_size, tokens), 0)
    named = [index_in[k : k + 1, :] for k in range(TOP)]
    hits = [(expert_rows == named[k]).astype(jnp.float32) for k in range(TOP)]
    before = (
        lax.broadcasted_iota(jnp.int32, (tokens, tokens), 0)
        < lax.broadcasted_iota(jnp.int32, (tokens, tokens), 1)
    ).astype(jnp.bfloat16)
    earlier = jnp.dot(
        (hits[0] + hits[1]).astype(jnp.bfloat16), before, preferred_element_type=jnp.float32
    )
    ranks = [
        jnp.sum(earlier * hits[0], axis=0, keepdims=True),
        jnp.sum((earlier + hits[0]) * hits[1], axis=0, keepdims=True),
    ]
    targets = []
    for k in range(TOP):
        rank = ranks[k].astype(jnp.int32)
        half_no = sum((rank >= part * i).astype(jnp.int32) for i in range(1, HALVES))
        targets.append((half_no * ep_size + named[k] - half_no) * part + rank)
    slot_rows = lax.broadcasted_iota(jnp.int32, (slots, tokens), 0)
    picks = jnp.logical_or(slot_rows == targets[0], slot_rows == targets[1])
    outgoing[...] = jnp.dot(
        picks.astype(jnp.bfloat16), x_in[...], preferred_element_type=jnp.float32
    ).astype(jnp.bfloat16)
    total_share = share_in[0:1, :] + share_in[1:2, :]
    row_id = lax.broadcasted_iota(jnp.int32, (tokens, tokens), 0)
    packed = jnp.zeros((tokens, tokens), jnp.float32)
    packed = jnp.where(row_id == 0, targets[0].astype(jnp.float32), packed)
    packed = jnp.where(row_id == 1, targets[1].astype(jnp.float32), packed)
    packed = jnp.where(row_id == 2, share_in[0:1, :] / total_share, packed)
    packed = jnp.where(row_id == 3, share_in[1:2, :] / total_share, packed)
    columns[...] = packed.T

    ext[pl.ds(REACH, length), :] = mix_in[...].astype(jnp.float32)
    group = (tp * chans) // group_size
    window = jnp.where(group == 0, 2, jnp.where(group == 1, 4, jnp.where(group == 2, 8, 16)))

    def window_sum(first, count):
        running = ext[pl.ds(REACH + first, count), :]
        for lag in range(1, REACH):
            running = running + jnp.where(
                lag < window, ext[pl.ds(REACH + first - lag, count), :], 0.0
            )
        return running

    inverse_window = jnp.where(
        group == 0, 0.5, jnp.where(group == 1, 0.25, jnp.where(group == 2, 0.125, 0.0625))
    )
    def pool(piece):
        at, size = mix.rows(piece)
        for first in range(at, at + size, min(64, size)):
            skip = REACH if first == 0 else 0
            begin, count = first + skip, min(64, size) - skip
            if count:
                pg[y, core, pl.ds(begin, count), :] = (
                    window_sum(begin, count) * inverse_window - ext[pl.ds(REACH + begin, count), :]
                ).astype(jnp.bfloat16)

    pl.semaphore_wait(barrier, ep_size - 1 + 3)

    halo_copy = pltpu.make_async_remote_copy(
        src_ref=mix_in.at[pl.ds(length - REACH, REACH), :],
        dst_ref=halo,
        send_sem=halo_sem.at[0],
        recv_sem=halo_sem.at[1],
        device_id=(lax.rem(ep + 1, ep_size), tp),
        device_id_type=MESH,
    )
    halo_copy.start()

    my_set = 0
    for bound in bounds[1:-1]:
        my_set = my_set + jnp.where(ep >= bound, 1, 0)

    def dispatch():
        for half_no in range(HALVES):
            for away_z, away_x in far_first(ep_size // nx, nx):
                other = lax.rem(ep // nx + away_z, ep_size // nx) * nx + lax.rem(ep + away_x, nx)
                pltpu.make_async_remote_copy(
                    src_ref=outgoing.at[sent_block(half_no, other), :],
                    dst_ref=tg.at[y, core, my_block(half_no), :],
                    send_sem=disp_send,
                    recv_sem=disp_recv.at[my_set * HALVES + half_no],
                    device_id=(other, tp),
                    device_id_type=MESH,
                ).start()

    def limit(piece, way):
        return half if (piece % 2 == 0) == (way == 0) else half - 1

    def arrival(piece, way, hop):
        return piece * (ny - 1) + way * limit(piece, 0) + hop - 1

    def part_of(hop):
        return [hop in hops for hops in PARTS].index(True)

    def piece_of(stream, origin, piece):
        return stream.buf.at[origin, core, pl.ds(*stream.rows(piece)), :]

    def ring_send(stream, piece, way, origin, hop):
        ref = piece_of(stream, origin, piece)
        pltpu.make_async_remote_copy(
            src_ref=ref,
            dst_ref=ref,
            send_sem=stream.send,
            recv_sem=stream.recv.at[arrival(piece, way, hop + 1)],
            device_id=(ep, up if way == 0 else down),
            device_id_type=MESH,
        ).start()

    def mate_copy(stream, piece, origin, hop):
        ref = piece_of(stream, origin, piece)
        pltpu.make_async_remote_copy(
            src_ref=ref,
            dst_ref=ref,
            send_sem=stream.mate_send,
            recv_sem=stream.mate_recv.at[piece // 2, part_of(hop)],
            device_id=(ep, mate),
            device_id_type=MESH,
        ).start()

    def origin_of(way, hop):
        return lax.rem(y + ny - hop, ny) if way == 0 else lax.rem(y + hop, ny)

    def move(stream, piece, hop):
        if hop == 0:
            for way in range(2):
                if limit(piece, way) > 0:
                    ring_send(stream, piece, way, y, 0)
            mate_copy(stream, piece, y, 0)
            return
        for way in range(2):
            if hop > limit(piece, way):
                continue
            origin = origin_of(way, hop)
            ref = piece_of(stream, origin, piece)
            pltpu.make_async_copy(ref, ref, stream.recv.at[arrival(piece, way, hop)]).wait()
            if hop < limit(piece, way):
                ring_send(stream, piece, way, origin, hop)
            mate_copy(stream, piece, origin, hop)

    def mate_wait(stream, group_no, part_no):
        origins = sum(1 if hop in (0, half) else 2 for hop in PARTS[part_no])
        ref = stream.buf.at[pl.ds(0, origins), 0, stream.group(group_no), :]
        pltpu.make_async_copy(ref, ref, stream.mate_recv.at[group_no, part_no]).wait()

    def origins_of(part_no):
        found = []
        for hop in PARTS[part_no]:
            found += [y] if hop == 0 else [origin_of(0, hop)]
            found += [origin_of(1, hop)] if 0 < hop < half else []
        return found

    def gathered(stream, group_no, part_no, totals, term):
        mate_wait(stream, group_no, part_no)
        at = stream.group(group_no)
        sums = [0.0] * len(totals)
        for origin in origins_of(part_no):
            sums = [a + b for a, b in zip(sums, term(origin, at))]
        for total, value in zip(totals, sums):
            total[at, :] = value if part_no == 0 else total[at, :] + value

    def rows_of(origin, size):
        return pl.ds(pl.multiple_of(origin * size, size), size)

    def mix_term(origin, at):
        a = jnp.concatenate([pg[origin, 0, at, :], pg[origin, 1, at, :]], axis=1)
        return [jnp.dot(a, mw[rows_of(origin, 2 * chans), :], preferred_element_type=jnp.float32)]

    def token_term(origin, at):
        scaled, sums = [], 0.0
        for j in range(2):
            x = tg[origin, j, at, :].astype(jnp.float32)
            lanes = pl.ds(pl.multiple_of((origin * 2 + j) * feats, feats), feats)
            scaled.append((x * gain_in[:, lanes]).astype(jnp.bfloat16))
            sq = x * x
            for q in range(0, feats, 128):
                sums = sums + sq[:, q : q + 128]
        got = jnp.dot(
            jnp.concatenate(scaled, axis=1),
            wgu[rows_of(origin, 2 * feats), :],
            preferred_element_type=jnp.float32,
        )
        return [got, sums]

    def down_term(origin, at):
        a = jnp.concatenate([hg[origin, 0, at, :], hg[origin, 1, at, :]], axis=1)
        return [jnp.dot(a, wd[rows_of(origin, 2 * hid), :], preferred_element_type=jnp.float32)]

    def activate(ch):
        at = tok.group(ch)
        total = jnp.sum(squares[at, :], axis=1, keepdims=True)
        inverse = lax.rsqrt(total / (feats * tp_size) + EPS)
        gate = acc_t[at, pl.ds(0, hid)] * inverse
        upper = acc_t[at, pl.ds(hid, hid)] * inverse
        hg[y, core, at, :] = (gate / (1.0 + jnp.exp(-gate)) * upper).astype(jnp.bfloat16)

    def inside(device, ch):
        g = ch // HALVES
        return jnp.logical_and(device >= bounds[g], device < bounds[g + 1])

    def dispatched(ch):
        base, rows = tok.group_first[ch], chunks[ch]
        mine = inside(ep, ch)

        @pl.when(mine)
        def _():
            if rows > part:
                ref = tg.at[0, 0, pl.ds(base, rows - part), :]
                pltpu.make_async_copy(ref, ref, disp_recv.at[ch]).wait()
            tg[y, core, chunk_block(ch, ep), :] = outgoing[sent_block(ch % HALVES, ep), :]

        @pl.when(jnp.logical_not(mine))
        def _():
            ref = tg.at[0, 0, pl.ds(base, rows), :]
            pltpu.make_async_copy(ref, ref, disp_recv.at[ch]).wait()

    def give_back(ch):
        at = tok.group(ch)
        produced[at, :] = acc_d[at, :].astype(jnp.bfloat16)
        g, half_no = ch // HALVES, ch % HALVES

        def one(i, carry):
            other = bounds[g] + lax.rem(ep + i, sources[g])

            @pl.when(other != ep)
            def _():
                pltpu.make_async_remote_copy(
                    src_ref=produced.at[chunk_block(ch, other), :],
                    dst_ref=returned.at[sent_block(half_no, ep), :],
                    send_sem=ret_send,
                    recv_sem=ret_recv,
                    device_id=(other, tp),
                    device_id_type=MESH,
                ).start()

            return carry

        lax.fori_loop(0, sources[g], one, 0)

        @pl.when(inside(ep, ch))
        def _():
            returned[sent_block(half_no, ep), :] = produced[chunk_block(ch, ep), :]

    def find_takes():
        slot_lanes = lax.broadcasted_iota(jnp.int32, (tokens, slots), 1)
        for k in range(TOP):
            takes[k] = (columns[:, k : k + 1].astype(jnp.int32) == slot_lanes).astype(jnp.bfloat16)

    def first_rows():
        halo_copy.wait_recv()
        ext[pl.ds(0, REACH), :] = jnp.where(ep == 0, 0.0, halo[...].astype(jnp.float32))
        position = ep * length + lax.broadcasted_iota(jnp.int32, (REACH, chans), 0)
        counts = jnp.minimum(position + 1, window).astype(jnp.float32)
        pg[y, core, pl.ds(0, REACH), :] = (
            window_sum(0, REACH) / counts - ext[pl.ds(REACH, REACH), :]
        ).astype(jnp.bfloat16)

    streams = {"m": mix, "t": tok, "h": hdn}
    weights = {"mc": [0], "tc": [1, 2], "hc": [3]}
    for entry in order:
        kind = entry[0]
        for i in weights.pop(kind, ()):
            w_copies[i].wait()
        if kind in streams:
            move(streams[kind], entry[1], entry[2])
        elif kind == "disp":
            dispatch()
        elif kind == "take":
            find_takes()
        elif kind == "pool":
            pool(entry[1])
        elif kind == "first":
            first_rows()
        elif kind == "got":
            dispatched(entry[1])
        elif kind == "mc":
            gathered(mix, entry[1], entry[2], [acc_m], mix_term)
        elif kind == "mo":
            mixed_out[...] = acc_m[...].astype(jnp.bfloat16)
        elif kind == "tc":
            gathered(tok, entry[1], entry[2], [acc_t, squares], token_term)
        elif kind == "act":
            activate(entry[1])
        elif kind == "hc":
            gathered(hdn, entry[1], entry[2], [acc_d], down_term)
        elif kind == "ret":
            give_back(entry[1])

    halo_copy.wait_send()
    others = pl.ds(0, slots - cap)
    pltpu.make_async_copy(outgoing.at[others, :], outgoing.at[others, :], disp_send).wait()
    pltpu.make_async_copy(produced.at[others, :], produced.at[others, :], ret_send).wait()
    for stream in streams.values():
        ref = stream.buf.at[pl.ds(0, ny - 1), 0, :, :]
        pltpu.make_async_copy(ref, ref, stream.send).wait()
        ref = stream.buf.at[:, 0, :, :]
        pltpu.make_async_copy(ref, ref, stream.mate_send).wait()

    pltpu.make_async_copy(returned.at[others, :], returned.at[others, :], ret_recv).wait()
    rows = 0.0
    for k in range(TOP):
        picked = jnp.dot(takes[k], returned[...], preferred_element_type=jnp.float32)
        rows = rows + picked * columns[:, TOP + k : TOP + k + 1]
    rows_out[...] = rows.astype(jnp.bfloat16)


SOURCES = (8, 8, 8, 8)
ORDER = (
    ("disp",), ("pool", 1), ("pool", 3), ("pool", 2), ("m", 1, 0), ("m", 3, 0), ("pool", 0),
    ("first",), ("m", 2, 0), ("m", 0, 0), ("m", 1, 1), ("m", 3, 1), ("m", 2, 1), ("m", 0, 1),
    ("take",), ("got", 0), ("t", 0, 0), ("got", 2), ("t", 1, 0), ("t", 4, 0), ("t", 5, 0),
    ("got", 1), ("t", 2, 0), ("t", 3, 0), ("got", 3), ("t", 7, 0), ("t", 1, 1), ("t", 0, 1),
    ("t", 6, 0), ("t", 5, 1), ("t", 3, 1), ("t", 2, 1), ("t", 4, 1), ("t", 1, 2), ("t", 0, 2),
    ("tc", 1, 0), ("t", 6, 1), ("t", 5, 2), ("t", 7, 1), ("t", 3, 2), ("tc", 2, 0), ("t", 2, 2),
    ("t", 4, 2), ("t", 0, 3), ("t", 1, 3), ("t", 6, 2), ("tc", 0, 0), ("t", 7, 2), ("t", 3, 3),
    ("t", 2, 3), ("tc", 0, 1), ("t", 5, 3), ("t", 4, 3), ("t", 1, 4), ("t", 0, 4), ("m", 1, 2),
    ("t", 6, 3), ("t", 7, 3), ("tc", 0, 2), ("act", 0), ("tc", 3, 0), ("h", 1, 0), ("t", 3, 4),
    ("h", 0, 0), ("t", 2, 4), ("tc", 1, 1), ("m", 2, 2), ("t", 5, 4), ("t", 4, 4), ("tc", 3, 1),
    ("tc", 2, 1), ("m", 3, 2), ("tc", 1, 2), ("act", 1), ("h", 2, 0), ("tc", 2, 2), ("act", 2),
    ("h", 4, 0), ("t", 6, 4), ("t", 7, 4), ("h", 5, 0), ("h", 3, 0), ("h", 1, 1), ("h", 0, 1),
    ("tc", 3, 2), ("act", 3), ("h", 7, 0), ("h", 6, 0), ("h", 2, 1), ("h", 4, 1), ("mc", 0, 0),
    ("h", 5, 1), ("h", 3, 1), ("h", 1, 2), ("h", 0, 2), ("mc", 1, 0), ("h", 7, 1), ("h", 6, 1),
    ("h", 2, 2), ("h", 4, 2), ("h", 5, 2), ("hc", 1, 0), ("hc", 2, 0), ("h", 3, 2), ("h", 1, 3),
    ("h", 0, 3), ("h", 7, 2), ("hc", 3, 0), ("h", 6, 2), ("m", 0, 2), ("h", 4, 3), ("h", 2, 3),
    ("hc", 0, 0), ("h", 5, 3), ("h", 3, 3), ("h", 1, 4), ("hc", 0, 1), ("m", 3, 3), ("m", 2, 3),
    ("h", 0, 4), ("h", 7, 3), ("h", 6, 3), ("hc", 1, 1), ("m", 1, 3), ("hc", 0, 2), ("ret", 0),
    ("h", 4, 4), ("h", 5, 4), ("m", 0, 3), ("hc", 2, 1), ("h", 3, 4), ("h", 2, 4), ("hc", 2, 2),
    ("ret", 2), ("h", 7, 4), ("h", 6, 4), ("hc", 1, 2), ("ret", 1), ("mc", 0, 1), ("m", 1, 4),
    ("hc", 3, 1), ("mc", 1, 1), ("hc", 3, 2), ("ret", 3), ("m", 0, 4), ("m", 3, 4), ("m", 2, 4),
    ("mc", 1, 2), ("mc", 0, 2), ("mo",),
)


def solution(mesh):
    ep_size, tp_size = mesh.shape["ep"], mesh.shape["tp"]
    ny = tp_size // 2
    half = ny // 2

    def shards(mix_input, mix_weight, expert_input, expert_index, route_share, norm_gain, gate_weight, up_weight, down_weight):
        length, chans = mix_input.shape
        tokens, feats = expert_input.shape
        slots = 2 * tokens * TOP
        width = mix_weight.shape[1]
        hid = gate_weight.shape[2]
        vmem, dma = pltpu.VMEM, pltpu.SemaphoreType.DMA
        bf16, f32 = jnp.bfloat16, jnp.float32

        sources = SOURCES if ep_size == sum(SOURCES) else (ep_size // len(SOURCES),) * len(SOURCES)
        chunks = len(sources) * HALVES

        def stream_sems(groups):
            return [dma, dma((2 * groups * (ny - 1),)), dma, dma((groups, len(PARTS)))]

        here = pl.BlockSpec(memory_space=pltpu.VMEM)
        there = pl.BlockSpec(memory_space=pltpu.HBM)
        flops = 2 * (length * chans * tp_size * width + slots * (feats * tp_size * 2 * hid + hid * tp_size * width))
        call = pl.pallas_call(
            functools.partial(
                kernel, ep_size, tp_size, chans * tp_size // 4, sources, ORDER
            ),
            name="mixer_and_experts",
            out_shape=(
                jax.ShapeDtypeStruct((length, width), bf16),
                jax.ShapeDtypeStruct((tokens, width), bf16),
            ),
            in_specs=[there] * 9,
            out_specs=(here, here),
            scratch_shapes=[
                vmem((length, chans), bf16),
                vmem((tokens, feats), bf16),
                vmem((TOP, tokens), jnp.int32),
                vmem((TOP, tokens), f32),
                vmem((1, feats * tp_size), f32),
                vmem(mix_weight.shape, bf16),
                vmem((feats * tp_size, 2 * hid), bf16),
                vmem(down_weight.shape[1:], bf16),
                vmem((length + REACH, chans), f32),
                vmem((REACH, chans), bf16),
                vmem((ny, 2, length, chans), bf16),
                vmem((ny, 2, slots, feats), bf16),
                vmem((ny, 2, slots, hid), bf16),
                vmem((slots, feats), bf16),
                vmem((slots, width), bf16),
                vmem((slots, width), bf16),
                vmem((length, width), f32),
                vmem((slots, 2 * hid), f32),
                vmem((slots, width), f32),
                vmem((slots, 128), f32),
                vmem((tokens, tokens), f32),
                vmem((TOP, tokens, slots), bf16),
                dma((5,)),
                dma((4,)),
                dma((2,)),
                dma,
                dma((chunks,)),
                dma,
                dma,
            ]
            + stream_sems(MIX_GROUPS)
            + stream_sems(chunks)
            + stream_sems(chunks),
            compiler_params=pltpu.CompilerParams(
                collective_id=0, has_side_effects=True, vmem_limit_bytes=24 * 1024 * 1024
            ),
            cost_estimate=pl.CostEstimate(flops=flops, bytes_accessed=8 * 1024 * 1024, transcendentals=0),
        )
        operands = (
            mix_input,
            expert_input,
            expert_index.T,
            route_share.T,
            norm_gain.reshape(1, -1),
            mix_weight,
            gate_weight[0],
            up_weight[0],
            down_weight[0],
        )
        return call(*(pltpu.with_memory_space_constraint(a, pltpu.HBM) for a in operands))

    placed = (
        P("ep", "tp"),
        P(None, "tp"),
        P("ep", "tp"),
        P("ep", None),
        P("ep", None),
        P(),
        P("ep", None, "tp"),
        P("ep", None, "tp"),
        P("ep", None, "tp"),
    )
    return jax.shard_map(
        shards,
        mesh=mesh,
        in_specs=placed,
        out_specs=(P("ep", "tp"), P("ep", "tp")),
        check_vma=False,
    )
```

```python
import functools

import jax
import jax.numpy as jnp
from jax import lax
from jax.experimental import pallas as pl
from jax.experimental.pallas import tpu as pltpu
from jax.sharding import PartitionSpec as P

MESH = pl.DeviceIdType.MESH
TOP = 2
REACH = 16
EPS = 1e-06
MIX_GROUPS = 2
PARTS = ((0, 1), (2, 3), (4,))
NX = 4
HALVES = 1


class Stream:
    def __init__(self, buf, group_rows, sems):
        self.buf = buf
        self.group_rows = group_rows
        self.group_first = [sum(group_rows[:g]) for g in range(len(group_rows))]
        self.send, self.recv, self.mate_send, self.mate_recv = sems

    def group(self, g):
        return pl.ds(self.group_first[g], self.group_rows[g])

    def rows(self, piece):
        size = self.group_rows[piece // 2] // 2
        return self.group_first[piece // 2] + (piece % 2) * size, size


def far_first(nz, nx):
    def hops(offset):
        return min(offset[0], nz - offset[0]) + min(offset[1], nx - offset[1])

    offsets = [(z, x) for z in range(nz) for x in range(nx) if z or x]
    return sorted(offsets, key=lambda offset: (-hops(offset), offset))


def kernel(
    ep_size,
    tp_size,
    group_size,
    sources,
    order,
    mix_hbm,
    x_hbm,
    index_hbm,
    share_hbm,
    gain_hbm,
    mix_w,
    gate_w,
    up_w,
    down_w,
    mixed_out,
    rows_out,
    mix_in,
    x_in,
    index_in,
    share_in,
    gain_in,
    mw,
    wgu,
    wd,
    ext,
    halo,
    pg,
    tg,
    hg,
    outgoing,
    produced,
    returned,
    acc_m,
    acc_t,
    acc_d,
    squares,
    columns,
    takes,
    in_sem,
    w_sem,
    halo_sem,
    disp_send,
    disp_recv,
    ret_send,
    ret_recv,
    m_send,
    m_recv,
    m_mate_send,
    m_mate_recv,
    t_send,
    t_recv,
    t_mate_send,
    t_mate_recv,
    h_send,
    h_recv,
    h_mate_send,
    h_mate_recv,
):
    ep = lax.axis_index("ep")
    tp = lax.axis_index("tp")
    ny = tp_size // 2
    half = ny // 2
    core = lax.rem(tp, 2)
    y = tp // 2
    up = lax.rem(tp + 2, tp_size)
    down = lax.rem(tp + tp_size - 2, tp_size)
    mate = tp + 1 - 2 * core
    tokens, feats = x_in.shape
    length, chans = mix_in.shape
    slots = outgoing.shape[0]
    cap = slots // ep_size
    nx = NX if ep_size % NX == 0 else 1
    hid = hg.shape[3]
    part = cap // HALVES
    sets = len(sources)
    bounds = [sum(sources[:g]) for g in range(sets + 1)]
    chunks = [sources[ch // HALVES] * part for ch in range(sets * HALVES)]

    mix = Stream(pg, [length // MIX_GROUPS] * MIX_GROUPS, (m_send, m_recv, m_mate_send, m_mate_recv))
    tok = Stream(tg, chunks, (t_send, t_recv, t_mate_send, t_mate_recv))
    hdn = Stream(hg, chunks, (h_send, h_recv, h_mate_send, h_mate_recv))

    def sent_block(half_no, expert):
        return pl.ds(pl.multiple_of((half_no * ep_size + expert) * part, part), part)

    def chunk_block(ch, source):
        first = sum(chunks[:ch])
        return pl.ds(pl.multiple_of(first + (source - bounds[ch // HALVES]) * part, part), part)

    def my_block(half_no):
        first = (bounds[0] * HALVES + half_no * sources[0] + ep - bounds[0]) * part
        for g in range(1, sets):
            at = (bounds[g] * HALVES + half_no * sources[g] + ep - bounds[g]) * part
            first = jnp.where(ep >= bounds[g], at, first)
        return pl.ds(pl.multiple_of(first, part), part)

    in_copies = [
        pltpu.make_async_copy(src, dst, in_sem.at[i])
        for i, (src, dst) in enumerate(
            (
                (index_hbm, index_in),
                (x_hbm, x_in),
                (share_hbm, share_in),
                (mix_hbm, mix_in),
                (gain_hbm, gain_in),
            )
        )
    ]
    for copy in in_copies:
        copy.start()
    w_copies = [
        pltpu.make_async_copy(mix_w, mw, w_sem.at[0]),
        pltpu.make_async_copy(gate_w, wgu.at[:, pl.ds(0, hid)], w_sem.at[1]),
        pltpu.make_async_copy(up_w, wgu.at[:, pl.ds(hid, hid)], w_sem.at[2]),
        pltpu.make_async_copy(down_w, wd, w_sem.at[3]),
    ]
    for copy in w_copies:
        copy.start()

    barrier = pltpu.get_barrier_semaphore()
    for other in (up, down, mate):
        pl.semaphore_signal(barrier, inc=1, device_id=(ep, other), device_id_type=MESH)

    def greet(i, carry):
        pl.semaphore_signal(
            barrier, inc=1, device_id=(lax.rem(ep + i, ep_size), tp), device_id_type=MESH
        )
        return carry

    lax.fori_loop(1, ep_size, greet, 0)

    for copy in in_copies[:2]:
        copy.wait()

    expert_rows = lax.broadcasted_iota(jnp.int32, (ep_size, tokens), 0)
    named = [index_in[k : k + 1, :] for k in range(TOP)]
    hits = [(expert_rows == named[k]).astype(jnp.float32) for k in range(TOP)]
    before = (
        lax.broadcasted_iota(jnp.int32, (tokens, tokens), 0)
        < lax.broadcasted_iota(jnp.int32, (tokens, tokens), 1)
    ).astype(jnp.bfloat16)
    earlier = jnp.dot(
        (hits[0] + hits[1]).astype(jnp.bfloat16), before, preferred_element_type=jnp.float32
    )
    ranks = [
        jnp.sum(earlier * hits[0], axis=0, keepdims=True),
        jnp.sum((earlier + hits[0]) * hits[1], axis=0, keepdims=True),
    ]
    targets = []
    for k in range(TOP):
        rank = ranks[k].astype(jnp.int32)
        half_no = sum((rank >= part * i).astype(jnp.int32) for i in range(1, HALVES))
        targets.append((half_no * ep_size + named[k] - half_no) * part + rank)
    slot_rows = lax.broadcasted_iota(jnp.int32, (slots, tokens), 0)
    picks = jnp.logical_or(slot_rows == targets[0], slot_rows == targets[1])
    outgoing[...] = jnp.dot(
        picks.astype(jnp.bfloat16), x_in[...], preferred_element_type=jnp.float32
    ).astype(jnp.bfloat16)
    group = (tp * chans) // group_size
    window = jnp.where(group == 0, 2, jnp.where(group == 1, 4, jnp.where(group == 2, 8, 16)))

    def window_sum(first, count):
        running = ext[pl.ds(REACH + first, count), :]
        for lag in range(1, REACH):
            running = running + jnp.where(
                lag < window, ext[pl.ds(REACH + first - lag, count), :], 0.0
            )
        return running

    inverse_window = jnp.where(
        group == 0, 0.5, jnp.where(group == 1, 0.25, jnp.where(group == 2, 0.125, 0.0625))
    )
    def pool(piece):
        at, size = mix.rows(piece)
        for first in range(at, at + size, min(64, size)):
            skip = REACH if first == 0 else 0
            begin, count = first + skip, min(64, size) - skip
            if count:
                pg[y, core, pl.ds(begin, count), :] = (
                    window_sum(begin, count) * inverse_window - ext[pl.ds(REACH + begin, count), :]
                ).astype(jnp.bfloat16)

    pl.semaphore_wait(barrier, ep_size - 1 + 3)

    halo_copy = pltpu.make_async_remote_copy(
        src_ref=mix_in.at[pl.ds(length - REACH, REACH), :],
        dst_ref=halo,
        send_sem=halo_sem.at[0],
        recv_sem=halo_sem.at[1],
        device_id=(lax.rem(ep + 1, ep_size), tp),
        device_id_type=MESH,
    )
    in_copies[3].wait()
    halo_copy.start()

    my_set = 0
    for bound in bounds[1:-1]:
        my_set = my_set + jnp.where(ep >= bound, 1, 0)

    def dispatch():
        for half_no in range(HALVES):
            for away_z, away_x in far_first(ep_size // nx, nx):
                other = lax.rem(ep // nx + away_z, ep_size // nx) * nx + lax.rem(ep + away_x, nx)
                pltpu.make_async_remote_copy(
                    src_ref=outgoing.at[sent_block(half_no, other), :],
                    dst_ref=tg.at[y, core, my_block(half_no), :],
                    send_sem=disp_send,
                    recv_sem=disp_recv.at[my_set * HALVES + half_no],
                    device_id=(other, tp),
                    device_id_type=MESH,
                ).start()

    def prepare():
        for i in (2, 4):
            in_copies[i].wait()
        ext[pl.ds(REACH, length), :] = mix_in[...].astype(jnp.float32)
        total_share = share_in[0:1, :] + share_in[1:2, :]
        row_id = lax.broadcasted_iota(jnp.int32, (tokens, tokens), 0)
        packed = jnp.zeros((tokens, tokens), jnp.float32)
        packed = jnp.where(row_id == 0, targets[0].astype(jnp.float32), packed)
        packed = jnp.where(row_id == 1, targets[1].astype(jnp.float32), packed)
        packed = jnp.where(row_id == 2, share_in[0:1, :] / total_share, packed)
        packed = jnp.where(row_id == 3, share_in[1:2, :] / total_share, packed)
        columns[...] = packed.T

    def limit(piece, way):
        return half if (piece % 2 == 0) == (way == 0) else half - 1

    def arrival(piece, way, hop):
        return piece * (ny - 1) + way * limit(piece, 0) + hop - 1

    def part_of(hop):
        return [hop in hops for hops in PARTS].index(True)

    def piece_of(stream, origin, piece):
        return stream.buf.at[origin, core, pl.ds(*stream.rows(piece)), :]

    def ring_send(stream, piece, way, origin, hop):
        ref = piece_of(stream, origin, piece)
        pltpu.make_async_remote_copy(
            src_ref=ref,
            dst_ref=ref,
            send_sem=stream.send,
            recv_sem=stream.recv.at[arrival(piece, way, hop + 1)],
            device_id=(ep, up if way == 0 else down),
            device_id_type=MESH,
        ).start()

    def mate_copy(stream, piece, origin, hop):
        ref = piece_of(stream, origin, piece)
        pltpu.make_async_remote_copy(
            src_ref=ref,
            dst_ref=ref,
            send_sem=stream.mate_send,
            recv_sem=stream.mate_recv.at[piece // 2, part_of(hop)],
            device_id=(ep, mate),
            device_id_type=MESH,
        ).start()

    def origin_of(way, hop):
        return lax.rem(y + ny - hop, ny) if way == 0 else lax.rem(y + hop, ny)

    def move(stream, piece, hop):
        if hop == 0:
            for way in range(2):
                if limit(piece, way) > 0:
                    ring_send(stream, piece, way, y, 0)
            mate_copy(stream, piece, y, 0)
            return
        for way in (piece % 2, 1 - piece % 2):
            if hop > limit(piece, way):
                continue
            origin = origin_of(way, hop)
            ref = piece_of(stream, origin, piece)
            pltpu.make_async_copy(ref, ref, stream.recv.at[arrival(piece, way, hop)]).wait()
            if hop < limit(piece, way):
                ring_send(stream, piece, way, origin, hop)
            mate_copy(stream, piece, origin, hop)

    def mate_wait(stream, group_no, part_no):
        origins = sum(1 if hop in (0, half) else 2 for hop in PARTS[part_no])
        ref = stream.buf.at[pl.ds(0, origins), 0, stream.group(group_no), :]
        pltpu.make_async_copy(ref, ref, stream.mate_recv.at[group_no, part_no]).wait()

    def origins_of(part_no):
        found = []
        for hop in PARTS[part_no]:
            found += [y] if hop == 0 else [origin_of(0, hop)]
            found += [origin_of(1, hop)] if 0 < hop < half else []
        return found

    def gathered(stream, group_no, part_no, totals, term):
        mate_wait(stream, group_no, part_no)
        at = stream.group(group_no)
        sums = [0.0] * len(totals)
        for origin in origins_of(part_no):
            sums = [a + b for a, b in zip(sums, term(origin, at))]
        for total, value in zip(totals, sums):
            total[at, :] = value if part_no == 0 else total[at, :] + value

    def rows_of(origin, size):
        return pl.ds(pl.multiple_of(origin * size, size), size)

    def mix_term(origin, at):
        a = jnp.concatenate([pg[origin, 0, at, :], pg[origin, 1, at, :]], axis=1)
        return [jnp.dot(a, mw[rows_of(origin, 2 * chans), :], preferred_element_type=jnp.float32)]

    def token_term(origin, at):
        scaled, sums = [], 0.0
        for j in range(2):
            x = tg[origin, j, at, :].astype(jnp.float32)
            lanes = pl.ds(pl.multiple_of((origin * 2 + j) * feats, feats), feats)
            scaled.append((x * gain_in[:, lanes]).astype(jnp.bfloat16))
            sq = x * x
            for q in range(0, feats, 128):
                sums = sums + sq[:, q : q + 128]
        got = jnp.dot(
            jnp.concatenate(scaled, axis=1),
            wgu[rows_of(origin, 2 * feats), :],
            preferred_element_type=jnp.float32,
        )
        return [got, sums]

    def down_term(origin, at):
        a = jnp.concatenate([hg[origin, 0, at, :], hg[origin, 1, at, :]], axis=1)
        return [jnp.dot(a, wd[rows_of(origin, 2 * hid), :], preferred_element_type=jnp.float32)]

    def activate(ch):
        at = tok.group(ch)
        total = jnp.sum(squares[at, :], axis=1, keepdims=True)
        inverse = lax.rsqrt(total / (feats * tp_size) + EPS)
        gate = acc_t[at, pl.ds(0, hid)] * inverse
        upper = acc_t[at, pl.ds(hid, hid)] * inverse
        hg[y, core, at, :] = (gate / (1.0 + jnp.exp(-gate)) * upper).astype(jnp.bfloat16)

    def inside(device, ch):
        g = ch // HALVES
        return jnp.logical_and(device >= bounds[g], device < bounds[g + 1])

    def dispatched(ch):
        base, rows = tok.group_first[ch], chunks[ch]
        mine = inside(ep, ch)

        @pl.when(mine)
        def _():
            if rows > part:
                ref = tg.at[0, 0, pl.ds(base, rows - part), :]
                pltpu.make_async_copy(ref, ref, disp_recv.at[ch]).wait()
            tg[y, core, chunk_block(ch, ep), :] = outgoing[sent_block(ch % HALVES, ep), :]

        @pl.when(jnp.logical_not(mine))
        def _():
            ref = tg.at[0, 0, pl.ds(base, rows), :]
            pltpu.make_async_copy(ref, ref, disp_recv.at[ch]).wait()

    def give_back(ch):
        at = tok.group(ch)
        produced[at, :] = acc_d[at, :].astype(jnp.bfloat16)
        g, half_no = ch // HALVES, ch % HALVES

        def one(i, carry):
            other = bounds[g] + lax.rem(ep + i, sources[g])

            @pl.when(other != ep)
            def _():
                pltpu.make_async_remote_copy(
                    src_ref=produced.at[chunk_block(ch, other), :],
                    dst_ref=returned.at[sent_block(half_no, ep), :],
                    send_sem=ret_send,
                    recv_sem=ret_recv,
                    device_id=(other, tp),
                    device_id_type=MESH,
                ).start()

            return carry

        lax.fori_loop(0, sources[g], one, 0)

        @pl.when(inside(ep, ch))
        def _():
            returned[sent_block(half_no, ep), :] = produced[chunk_block(ch, ep), :]

    def find_takes():
        slot_lanes = lax.broadcasted_iota(jnp.int32, (tokens, slots), 1)
        for k in range(TOP):
            takes[k] = (columns[:, k : k + 1].astype(jnp.int32) == slot_lanes).astype(jnp.bfloat16)

    def first_rows():
        halo_copy.wait_recv()
        ext[pl.ds(0, REACH), :] = jnp.where(ep == 0, 0.0, halo[...].astype(jnp.float32))
        position = ep * length + lax.broadcasted_iota(jnp.int32, (REACH, chans), 0)
        counts = jnp.minimum(position + 1, window).astype(jnp.float32)
        pg[y, core, pl.ds(0, REACH), :] = (
            window_sum(0, REACH) / counts - ext[pl.ds(REACH, REACH), :]
        ).astype(jnp.bfloat16)

    streams = {"m": mix, "t": tok, "h": hdn}
    weights = {"mc": [0], "tc": [1, 2], "hc": [3]}
    for entry in order:
        kind = entry[0]
        for i in weights.pop(kind, ()):
            w_copies[i].wait()
        if kind in streams:
            move(streams[kind], entry[1], entry[2])
        elif kind == "disp":
            dispatch()
            prepare()
        elif kind == "take":
            find_takes()
        elif kind == "pool":
            pool(entry[1])
        elif kind == "first":
            first_rows()
        elif kind == "got":
            dispatched(entry[1])
        elif kind == "mc":
            gathered(mix, entry[1], entry[2], [acc_m], mix_term)
        elif kind == "mo":
            mixed_out[...] = acc_m[...].astype(jnp.bfloat16)
        elif kind == "tc":
            gathered(tok, entry[1], entry[2], [acc_t, squares], token_term)
        elif kind == "act":
            activate(entry[1])
        elif kind == "hc":
            gathered(hdn, entry[1], entry[2], [acc_d], down_term)
        elif kind == "ret":
            give_back(entry[1])

    halo_copy.wait_send()
    others = pl.ds(0, slots - cap)
    pltpu.make_async_copy(outgoing.at[others, :], outgoing.at[others, :], disp_send).wait()
    pltpu.make_async_copy(produced.at[others, :], produced.at[others, :], ret_send).wait()
    for stream in streams.values():
        ref = stream.buf.at[pl.ds(0, ny - 1), 0, :, :]
        pltpu.make_async_copy(ref, ref, stream.send).wait()
        ref = stream.buf.at[:, 0, :, :]
        pltpu.make_async_copy(ref, ref, stream.mate_send).wait()

    pltpu.make_async_copy(returned.at[others, :], returned.at[others, :], ret_recv).wait()
    rows = 0.0
    for k in range(TOP):
        picked = jnp.dot(takes[k], returned[...], preferred_element_type=jnp.float32)
        rows = rows + picked * columns[:, TOP + k : TOP + k + 1]
    rows_out[...] = rows.astype(jnp.bfloat16)


SOURCES = (8, 8, 8, 8)
ORDER = (
    ("disp",), ("pool", 1), ("pool", 3), ("pool", 2), ("m", 1, 0), ("m", 3, 0), ("pool", 0),
    ("first",), ("m", 2, 0), ("m", 0, 0), ("m", 1, 1), ("m", 3, 1), ("m", 2, 1), ("m", 0, 1),
    ("take",), ("got", 0), ("t", 0, 0), ("got", 2), ("t", 1, 0), ("t", 4, 0), ("t", 5, 0),
    ("got", 1), ("t", 2, 0), ("t", 3, 0), ("got", 3), ("t", 7, 0), ("t", 1, 1), ("t", 0, 1),
    ("t", 6, 0), ("t", 5, 1), ("t", 3, 1), ("t", 2, 1), ("t", 4, 1), ("t", 1, 2), ("t", 0, 2),
    ("tc", 1, 0), ("t", 6, 1), ("t", 5, 2), ("t", 7, 1), ("t", 3, 2), ("tc", 2, 0), ("t", 2, 2),
    ("t", 4, 2), ("t", 0, 3), ("t", 1, 3), ("t", 6, 2), ("tc", 0, 0), ("t", 7, 2), ("t", 3, 3),
    ("t", 2, 3), ("tc", 0, 1), ("t", 5, 3), ("t", 4, 3), ("t", 1, 4), ("t", 0, 4), ("m", 1, 2),
    ("t", 6, 3), ("t", 7, 3), ("tc", 0, 2), ("act", 0), ("tc", 3, 0), ("h", 1, 0), ("t", 3, 4),
    ("h", 0, 0), ("t", 2, 4), ("tc", 1, 1), ("m", 2, 2), ("t", 5, 4), ("t", 4, 4), ("tc", 3, 1),
    ("tc", 2, 1), ("m", 3, 2), ("tc", 1, 2), ("act", 1), ("h", 2, 0), ("tc", 2, 2), ("act", 2),
    ("h", 4, 0), ("t", 6, 4), ("t", 7, 4), ("h", 5, 0), ("h", 3, 0), ("h", 1, 1), ("h", 0, 1),
    ("tc", 3, 2), ("act", 3), ("h", 7, 0), ("h", 6, 0), ("h", 2, 1), ("h", 4, 1), ("mc", 0, 0),
    ("h", 5, 1), ("h", 3, 1), ("h", 1, 2), ("h", 0, 2), ("mc", 1, 0), ("h", 7, 1), ("h", 6, 1),
    ("h", 2, 2), ("h", 4, 2), ("h", 5, 2), ("hc", 1, 0), ("hc", 2, 0), ("h", 3, 2), ("h", 1, 3),
    ("h", 0, 3), ("h", 7, 2), ("hc", 3, 0), ("h", 6, 2), ("m", 0, 2), ("h", 4, 3), ("h", 2, 3),
    ("hc", 0, 0), ("h", 5, 3), ("h", 3, 3), ("h", 1, 4), ("hc", 0, 1), ("m", 3, 3), ("m", 2, 3),
    ("h", 0, 4), ("h", 7, 3), ("h", 6, 3), ("hc", 1, 1), ("m", 1, 3), ("hc", 0, 2), ("ret", 0),
    ("h", 4, 4), ("h", 5, 4), ("m", 0, 3), ("hc", 2, 1), ("h", 3, 4), ("h", 2, 4), ("hc", 2, 2),
    ("ret", 2), ("h", 7, 4), ("h", 6, 4), ("hc", 1, 2), ("ret", 1), ("mc", 0, 1), ("m", 1, 4),
    ("hc", 3, 1), ("mc", 1, 1), ("hc", 3, 2), ("ret", 3), ("m", 0, 4), ("m", 3, 4), ("m", 2, 4),
    ("mc", 1, 2), ("mc", 0, 2), ("mo",),
)


def solution(mesh):
    ep_size, tp_size = mesh.shape["ep"], mesh.shape["tp"]
    ny = tp_size // 2
    half = ny // 2

    def shards(mix_input, mix_weight, expert_input, expert_index, route_share, norm_gain, gate_weight, up_weight, down_weight):
        length, chans = mix_input.shape
        tokens, feats = expert_input.shape
        slots = 2 * tokens * TOP
        width = mix_weight.shape[1]
        hid = gate_weight.shape[2]
        vmem, dma = pltpu.VMEM, pltpu.SemaphoreType.DMA
        bf16, f32 = jnp.bfloat16, jnp.float32

        sources = SOURCES if ep_size == sum(SOURCES) else (ep_size // len(SOURCES),) * len(SOURCES)
        chunks = len(sources) * HALVES

        def stream_sems(groups):
            return [dma, dma((2 * groups * (ny - 1),)), dma, dma((groups, len(PARTS)))]

        here = pl.BlockSpec(memory_space=pltpu.VMEM)
        there = pl.BlockSpec(memory_space=pltpu.HBM)
        flops = 2 * (length * chans * tp_size * width + slots * (feats * tp_size * 2 * hid + hid * tp_size * width))
        call = pl.pallas_call(
            functools.partial(
                kernel, ep_size, tp_size, chans * tp_size // 4, sources, ORDER
            ),
            name="mixer_and_experts",
            out_shape=(
                jax.ShapeDtypeStruct((length, width), bf16),
                jax.ShapeDtypeStruct((tokens, width), bf16),
            ),
            in_specs=[there] * 9,
            out_specs=(here, here),
            scratch_shapes=[
                vmem((length, chans), bf16),
                vmem((tokens, feats), bf16),
                vmem((TOP, tokens), jnp.int32),
                vmem((TOP, tokens), f32),
                vmem((1, feats * tp_size), f32),
                vmem(mix_weight.shape, bf16),
                vmem((feats * tp_size, 2 * hid), bf16),
                vmem(down_weight.shape[1:], bf16),
                vmem((length + REACH, chans), f32),
                vmem((REACH, chans), bf16),
                vmem((ny, 2, length, chans), bf16),
                vmem((ny, 2, slots, feats), bf16),
                vmem((ny, 2, slots, hid), bf16),
                vmem((slots, feats), bf16),
                vmem((slots, width), bf16),
                vmem((slots, width), bf16),
                vmem((length, width), f32),
                vmem((slots, 2 * hid), f32),
                vmem((slots, width), f32),
                vmem((slots, 128), f32),
                vmem((tokens, tokens), f32),
                vmem((TOP, tokens, slots), bf16),
                dma((5,)),
                dma((4,)),
                dma((2,)),
                dma,
                dma((chunks,)),
                dma,
                dma,
            ]
            + stream_sems(MIX_GROUPS)
            + stream_sems(chunks)
            + stream_sems(chunks),
            compiler_params=pltpu.CompilerParams(
                collective_id=0, has_side_effects=True, vmem_limit_bytes=24 * 1024 * 1024
            ),
            cost_estimate=pl.CostEstimate(flops=flops, bytes_accessed=8 * 1024 * 1024, transcendentals=0),
        )
        operands = (
            mix_input,
            expert_input,
            expert_index.T,
            route_share.T,
            norm_gain.reshape(1, -1),
            mix_weight,
            gate_weight[0],
            up_weight[0],
            down_weight[0],
        )
        return call(*(pltpu.with_memory_space_constraint(a, pltpu.HBM) for a in operands))

    placed = (
        P("ep", "tp"),
        P(None, "tp"),
        P("ep", "tp"),
        P("ep", None),
        P("ep", None),
        P(),
        P("ep", None, "tp"),
        P("ep", None, "tp"),
        P("ep", None, "tp"),
    )
    return jax.shard_map(
        shards,
        mesh=mesh,
        in_specs=placed,
        out_specs=(P("ep", "tp"), P("ep", "tp")),
        check_vma=False,
    )
```
